128 devices in a mesh: sp: 16 (over z, y), tp: 8 (over x, core).
Axes of the slice: x: 4, y: 4, z: 4, core: 2. Of those that a mesh axis runs over, the one named last changes fastest.
Arguments:
- inputs: bfloat16 [16384, 2048], P(('sp', 'tp')), may hold values from -90 to 90
- in_gain: float32 [2048], replicated, may hold values from 0.1 to 1.9
- w_query: bfloat16 [2048, 1024], replicated, may hold values from -2 to 2
- w_key: bfloat16 [2048, 128], replicated, may hold values from -2 to 2
- w_value: bfloat16 [2048, 128], replicated, may hold values from -0.125 to 0.125
- query_gain: float32 [64], replicated, may hold values from 0 to 8, as said below
- key_gain: float32 [64], replicated, may hold values from 0 to 8, as said below
- decay_sums: float32 [16384, 16], P('sp', 'tp'), may hold values from -2343 to 0, as said below
- w_out: bfloat16 [1024, 2048], replicated, may hold values from -0.1875 to 0.1875
Outputs:
- result: bfloat16 [16384, 2048], P(('sp', 'tp'))
The draws below stay inside these ranges and needn't reach their ends.
Inputs may be any that keep to these rules, and one draw needn't show every extreme that they name: `decay_sums`: along positions, each head's entries never rise. `query_gain`: every entry is positive. `key_gain`: every entry is positive.
All inputs are finite; a program needn't handle non-finite values.
Results may differ from the reference program's by a relative error of at most 0.015.
The reference program's roundings to bfloat16 on the way count: a program that leaves them out, or rounds other values in their place, can miss the bound.
Values may be sent and summed in bfloat16 or wider, within the bound.
A program may use at most 64 MiB of HBM per device.

```python
import math
import jax
import jax.numpy as jnp
from jax import lax

D = 2048
QUERY_HEADS = 16
DH = 64
KV = 2
TOK_DEV = 1024
SEQUENCE_LENGTH = 16384


def draw_inputs(key, part):
    key_noise, key_shift = jax.random.split(jax.random.fold_in(key, 13), 2)
    noise = jax.random.truncated_normal(key_noise, -5.0, 5.0, (SEQUENCE_LENGTH, D), jnp.float32)
    shift = jax.random.truncated_normal(key_shift, -4.0, 4.0, (SEQUENCE_LENGTH // TOK_DEV, D), jnp.float32)
    shifted = noise + jnp.repeat(shift, TOK_DEV, axis=0)
    return shifted.astype(jnp.bfloat16)


def draw_w_query(key, part):
    noise = jax.random.truncated_normal(jax.random.fold_in(key, 31), -6.0, 6.0, (D, QUERY_HEADS * DH), jnp.float32) * D ** (-0.5)
    return noise.astype(jnp.bfloat16)


def draw_w_key(key, part):
    noise = jax.random.truncated_normal(jax.random.fold_in(key, 32), -6.0, 6.0, (D, KV * DH), jnp.float32) * D ** (-0.5)
    return noise.astype(jnp.bfloat16)


def draw_query_gain(key, part):
    return jax.random.uniform(jax.random.fold_in(key, 11), (DH,), jnp.float32, 0.4, 1.6)


def draw_key_gain(key, part):
    return jax.random.uniform(jax.random.fold_in(key, 12), (DH,), jnp.float32, 0.4, 1.6)


def draw_decay_sums(key, part):
    random_part_keys = jax.random.split(jax.random.fold_in(key, 14), 7)
    order = jax.random.permutation(random_part_keys[0], QUERY_HEADS)
    fast_count = QUERY_HEADS // 2
    fast = (order < fast_count)[None, :]
    slow_rate = jax.random.uniform(random_part_keys[1], (1, QUERY_HEADS), jnp.float32, 0.2, 0.6) / SEQUENCE_LENGTH
    fast_rate = jax.random.uniform(random_part_keys[2], (1, QUERY_HEADS), jnp.float32, 1.0 / 60.0, 1.0 / 25.0)
    base_offset = jnp.where(fast, fast_rate, slow_rate)
    coarse_estimate = jax.random.uniform(random_part_keys[3], (SEQUENCE_LENGTH, QUERY_HEADS), jnp.float32, 0.3, 1.7)
    block_multiple = jnp.exp(jax.random.uniform(random_part_keys[4], (SEQUENCE_LENGTH // TOK_DEV, QUERY_HEADS), jnp.float32, -math.log(2.0), math.log(2.0)))
    block_multiple = jnp.repeat(block_multiple, TOK_DEV, axis=0)
    spike_position = jax.random.randint(random_part_keys[5], (3,), 0, SEQUENCE_LENGTH)
    spike_depth = jnp.log(jax.random.uniform(random_part_keys[6], (3, QUERY_HEADS), jnp.float32, 0.5, 0.8))
    match_count = (jnp.arange(SEQUENCE_LENGTH, dtype=jnp.int32)[:, None] == spike_position[None, :]).astype(jnp.float32)
    spike_list = jnp.dot(match_count, spike_depth, precision=lax.Precision.HIGHEST)
    step_log_gates = -base_offset * coarse_estimate * block_multiple + spike_list
    return jnp.cumsum(step_log_gates, axis=0)


def gaussian(rng, shape, spread, most, kind=jnp.bfloat16):
    drawn = jax.random.normal(rng, shape, jnp.float32) * spread
    return jnp.minimum(jnp.maximum(drawn, -most), most).astype(kind)


def setup_inputs(seed: int = 0) -> dict:
    arg_keys = jax.random.split(jax.random.key(seed), 10)
    inputs = draw_inputs(jax.random.fold_in(arg_keys[9], 71), 0)
    in_gain = jnp.clip(1.0 + 0.18 * jax.random.normal(arg_keys[1], (D,), jnp.float32), 0.1, 1.9)
    w_query = draw_w_query(jax.random.fold_in(arg_keys[9], 71), 0)
    w_key = draw_w_key(jax.random.fold_in(arg_keys[9], 71), 0)
    w_value = gaussian(arg_keys[4], (D, KV * DH), D ** -0.5, 0.125)
    query_gain = draw_query_gain(jax.random.fold_in(arg_keys[9], 71), 0)
    key_gain = draw_key_gain(jax.random.fold_in(arg_keys[9], 71), 0)
    decay_sums = draw_decay_sums(jax.random.fold_in(arg_keys[9], 71), 0)
    w_out = gaussian(arg_keys[8], (QUERY_HEADS * DH, D), (QUERY_HEADS * DH) ** -0.5, 0.1875)
    return dict(inputs=inputs, in_gain=in_gain, w_query=w_query, w_key=w_key, w_value=w_value, query_gain=query_gain, key_gain=key_gain, decay_sums=decay_sums, w_out=w_out)


epsilon = 1e-06

def rms_norm(vector, gain_vec):
    return vector * lax.rsqrt(lax.optimization_barrier(jnp.mean(vector * vector, axis=-1, keepdims=True)) + epsilon) * gain_vec

def reference(inputs, in_gain, w_query, w_key, w_value, query_gain, key_gain, decay_sums, w_out):
    length = inputs.shape[0]
    normed = rms_norm(inputs.astype(jnp.float32), in_gain).astype(jnp.bfloat16)
    queries = rms_norm(jnp.dot(normed, w_query, preferred_element_type=jnp.float32).reshape(length, QUERY_HEADS, DH), query_gain).astype(jnp.bfloat16)
    keys = rms_norm(jnp.dot(normed, w_key, preferred_element_type=jnp.float32).reshape(length, KV, DH), key_gain).astype(jnp.bfloat16)
    values = jnp.dot(normed, w_value, preferred_element_type=jnp.float32).astype(jnp.bfloat16).reshape(length, KV, DH)
    group_size = QUERY_HEADS // KV
    keys_wide = jnp.repeat(keys, group_size, axis=1).astype(jnp.float32)
    values_wide = jnp.repeat(values, group_size, axis=1).astype(jnp.float32)
    block_rows = math.gcd(length, 512)
    block_count = length // block_rows
    key_pos = jnp.arange(length, dtype=jnp.int32)
    key_decay = decay_sums.T
    score_scale = DH ** (-0.5)

    def attend_block(block_index):
        offset = (block_index * block_rows).astype(jnp.int32)
        query_rows = lax.dynamic_slice_in_dim(queries, offset, block_rows, 0).astype(jnp.float32)
        query_decay = lax.dynamic_slice_in_dim(decay_sums, offset, block_rows, 0)
        scores = jnp.einsum('qhd,khd->hqk', query_rows, keys_wide) * score_scale
        scores = scores + query_decay.T[:, :, None] - key_decay[:, None, :]
        query_pos = offset + jnp.arange(block_rows, dtype=jnp.int32)
        visible = key_pos[None, :] <= query_pos[:, None]
        scores = jnp.where(visible[None], scores, -1e+30)
        peak = lax.optimization_barrier(jnp.max(scores, axis=-1, keepdims=True))
        weights_exp = jnp.where(visible[None], jnp.exp(scores - peak), 0.0)
        total = lax.optimization_barrier(jnp.sum(weights_exp, axis=-1))
        rounded = lax.optimization_barrier(weights_exp.astype(jnp.bfloat16)).astype(jnp.float32)
        mixed = jnp.einsum('hqk,khd->qhd', rounded, values_wide)
        return (mixed / total.T[:, :, None]).astype(jnp.bfloat16)
    blocks = lax.map(attend_block, jnp.arange(block_count, dtype=jnp.int32))
    attended = blocks.reshape(length, QUERY_HEADS * DH)
    return jnp.dot(attended, w_out, preferred_element_type=jnp.float32).astype(jnp.bfloat16)
```

```python
import functools

import jax
import jax.numpy as jnp
from jax import lax
from jax.experimental import pallas as pl
from jax.experimental.pallas import tpu as pltpu
from jax.sharding import Mesh
from jax.sharding import PartitionSpec as P

f32 = jnp.float32
bf = jnp.bfloat16
LOG2E = 1.4426950408889634
EPS = 1e-06
MESH = pl.DeviceIdType.MESH
VM = pl.BlockSpec(memory_space=pltpu.VMEM)


def split3(x):
    high = x.astype(bf).astype(f32)
    rest = x - high
    mid = rest.astype(bf).astype(f32)
    return high, mid, rest - mid


def head_norm(flat, heads, gain):
    x = flat.reshape(heads, 64, flat.shape[1])
    scale = lax.rsqrt(jnp.mean(x * x, axis=1, keepdims=True) + EPS)
    return (x * scale * gain[None]).reshape(flat.shape)


def project_kernel(x_ref, gain_ref, wk_ref, wv_ref, wq_ref, qg_ref, kg_ref, q_ref, kv_ref, norm_ref):
    step = pl.program_id(0)

    @pl.when(step == 0)
    def _():
        x = x_ref[...].astype(f32)
        scale = lax.rsqrt(jnp.mean(x * x, axis=1, keepdims=True) + EPS)
        norm_ref[...] = (x * scale * gain_ref[...]).astype(bf)
        keys = jnp.dot(norm_ref[...], wk_ref[...], preferred_element_type=f32)
        values = jnp.dot(norm_ref[...], wv_ref[...], preferred_element_type=f32)
        keys = head_norm(keys.T, 2, kg_ref[...]).astype(bf)
        values = values.T.astype(bf)
        for g in range(2):
            kv_ref[g, 0:64] = keys[g * 64 : (g + 1) * 64]
            kv_ref[g, 64:128] = values[g * 64 : (g + 1) * 64]

    queries = jnp.dot(norm_ref[...], wq_ref[...], preferred_element_type=f32)
    queries = head_norm(queries.T, wq_ref.shape[1] // 64, qg_ref[...])
    q_ref[...] = (queries * (LOG2E / 8)).astype(bf)


def project(x, gain, wk, wv, wq, qg, kg):
    cols = 256
    whole = lambda shape: pl.BlockSpec(shape, lambda j: (0,) * len(shape))
    return pl.pallas_call(
        project_kernel,
        grid=(1024 // cols,),
        out_shape=[jax.ShapeDtypeStruct((1024, 128), bf), jax.ShapeDtypeStruct((2, 128, 128), bf)],
        in_specs=[
            whole((128, 2048)),
            whole((1, 2048)),
            whole((2048, 128)),
            whole((2048, 128)),
            pl.BlockSpec((2048, cols), lambda j: (0, j)),
            whole((64, 1)),
            whole((64, 1)),
        ],
        out_specs=[pl.BlockSpec((cols, 128), lambda j: (j, 0)), whole((2, 128, 128))],
        scratch_shapes=[pltpu.VMEM((128, 2048), bf)],
        compiler_params=pltpu.CompilerParams(vmem_limit_bytes=24 * 1024 * 1024),
        cost_estimate=pl.CostEstimate(
            flops=2 * 128 * 2048 * 1280, bytes_accessed=6 * 1024 * 1024, transcendentals=0
        ),
        name="project",
    )(x, gain, wk, wv, wq, qg, kg)


def line_of(c, a, b):
    a, b = lax.rem(a + 8, 4), lax.rem(b + 8, 4)
    return (1 - c) * (4 * b + a) + c * (4 * a + b)


def gather_kernel(q_ref, kv_ref, d_ref, part_ref, all_ref, dec_ref, *sems):
    ks_send, ks_recv, ds_send, ds_recv, q_send, q_recv, r_send, r_recv, s_send, s_recv = sems
    z, y, x, c = (lax.axis_index(n) for n in ("z", "y", "x", "c"))
    g = x // 2
    line = 4 * z + y
    tp = 2 * x + c
    mine = (x - 2 * g) * 2 + c
    mirror = (3 - z, 3 - y, 3 - x, 1 - c)
    a = (1 - c) * y + c * z
    b = (1 - c) * z + c * y

    def at_ab(pa, pb):
        pa, pb = lax.rem(pa + 8, 4), lax.rem(pb + 8, 4)
        return ((1 - c) * pb + c * pa, (1 - c) * pa + c * pb, x, c)

    def in_line(t):
        t = lax.rem(t + 8, 8)
        return (z, y, t // 2, lax.rem(t, 2))

    barrier = pltpu.get_barrier_semaphore()
    peers = [in_line(tp + k) for k in range(1, 8)] + [mirror]
    peers += [at_ab(a + 1, b), at_ab(a - 1, b), at_ab(a, b + 1), at_ab(a, b - 1)]
    for peer in peers:
        pl.semaphore_signal(barrier, inc=1, device_id=peer, device_id_type=MESH)

    all_ref[line, tp, 0:128] = kv_ref[g]
    dec_ref[mine] = d_ref[...]
    pl.semaphore_wait(barrier, len(peers))

    started = []

    def send(src, dst, send_sem, recv_sem, peer):
        copy = pltpu.make_async_remote_copy(
            src_ref=src,
            dst_ref=dst,
            send_sem=send_sem,
            recv_sem=recv_sem,
            device_id=peer,
            device_id_type=MESH,
        )
        copy.start()
        started.append(copy)
        return copy

    decays = []
    for k in range(1, 4):
        t = lax.rem(mine + k, 4)
        peer = (z, y, 2 * g + t // 2, lax.rem(t, 2))
        decays.append(send(d_ref, dec_ref.at[mine], ds_send.at[k], ds_recv.at[k], peer))
    pieces = []
    for k in range(1, 8):
        t = lax.rem(tp + k, 8)
        pieces.append(
            send(
                kv_ref.at[t // 4],
                all_ref.at[line, tp, pl.ds(0, 128)],
                ks_send.at[k],
                ks_recv.at[k],
                in_line(tp + k),
            )
        )
    q_copy = send(q_ref.at[pl.ds((1 - g) * 512, 512)], part_ref, q_send, q_recv, mirror)

    for copy in decays:
        copy.wait_recv()
    row8 = lax.broadcasted_iota(jnp.int32, (8, 128), 0)
    ones = jnp.where(row8 < 3, 1.0, 0.0).astype(f32)
    for p in range(8):
        cols = slice(p * 128, (p + 1) * 128)
        value = jnp.concatenate([dec_ref[q, :, cols] for q in range(4)], axis=0) * LOG2E
        all_ref[line, p, 128:160] = jnp.concatenate([*split3(value), ones], axis=0).astype(bf)
    for copy in pieces:
        copy.wait_recv()

    def block(ln, sub):
        return all_ref.at[ln, pl.ds(4 * c + 2 * sub, 2)]

    def ring_send(ln, sub, slot, peer):
        return send(block(ln, sub), block(ln, sub), r_send.at[slot], r_recv.at[slot], peer)

    sibling = (z, y, x, 1 - c)
    shared = []

    def share(ln, slot):
        half = all_ref.at[ln, pl.ds(4 * c, 4)]
        shared.append(send(half, half, s_send.at[slot], s_recv.at[slot], sibling))

    def ring_start(step, ln, up, down):
        right = [ring_send(ln, sub, step * 6 + sub, up) for sub in range(2)]
        left = [ring_send(ln, sub, step * 6 + 2 + sub, down) for sub in range(2)]
        return right, left

    def ring_relay(step, copies, ln_left, ln_right, up, down):
        right, left = copies
        right[0].wait_recv()
        first = ring_send(ln_left, 0, step * 6 + 4, up)
        left[1].wait_recv()
        second = ring_send(ln_right, 1, step * 6 + 5, down)
        right[1].wait_recv()
        left[0].wait_recv()
        return first, second

    up_a, down_a = at_ab(a + 1, b), at_ab(a - 1, b)
    up_b, down_b = at_ab(a, b + 1), at_ab(a, b - 1)
    own = [line_of(c, a, b), line_of(c, a - 1, b), line_of(c, a + 1, b), line_of(c, a + 2, b)]
    along_a = (0, -1, 1, 2)

    first_copies = ring_start(0, own[0], up_a, down_a)
    second = [ring_start(1, own[0], up_b, down_b)]
    relays = ring_relay(0, first_copies, own[1], own[2], up_a, down_a)
    for j in (1, 2):
        second.append(ring_start(1 + j, own[j], up_b, down_b))
        share(own[j], j)
    for copy in relays:
        copy.wait_recv()
    second.append(ring_start(4, own[3], up_b, down_b))
    share(own[3], 3)
    last = []
    for j in range(4):
        left_line = line_of(c, a + along_a[j], b - 1)
        right_line = line_of(c, a + along_a[j], b + 1)
        last.append(ring_relay(1 + j, second[j], left_line, right_line, up_b, down_b))
        share(left_line, 4 + 3 * j)
        share(right_line, 5 + 3 * j)
    for j in range(4):
        for copy in last[j]:
            copy.wait_recv()
        share(line_of(c, a + along_a[j], b + 2), 6 + 3 * j)
    q_copy.wait_recv()
    for copy in shared:
        copy.wait_recv()
    for copy in started:
        copy.wait_send()


def gather(q, kv, d):
    dma = lambda *n: pltpu.SemaphoreType.DMA(n)
    return pl.pallas_call(
        gather_kernel,
        out_shape=[jax.ShapeDtypeStruct((512, 128), bf), jax.ShapeDtypeStruct((16, 8, 160, 128), bf)],
        in_specs=[VM, VM, VM],
        out_specs=[VM, VM],
        scratch_shapes=[
            pltpu.VMEM((4, 2, 1024), f32),
            dma(8),
            dma(8),
            dma(4),
            dma(4),
            pltpu.SemaphoreType.DMA,
            pltpu.SemaphoreType.DMA,
            dma(30),
            dma(30),
            dma(16),
            dma(16),
        ],
        compiler_params=pltpu.CompilerParams(
            collective_id=0, has_side_effects=True, vmem_limit_bytes=24 * 1024 * 1024
        ),
        name="gather",
    )(q, kv, d)


def load_keys(kvd, piece, ref_d, ones):
    blk = kvd[piece]
    dec = blk[128:160].astype(f32)
    rel = dec[0:8] + dec[8:16] + dec[16:24] - ref_d
    rows = jnp.concatenate([*split3(rel), ones], axis=0).astype(bf)
    full = jnp.concatenate([blk[0:64], rows, jnp.zeros((32, 128), bf)], axis=0)
    return full.T, blk[64:128]


def attend_kernel(bounded, chunk_pieces, tile, q_ref, part_ref, kvd_ref, oo_ref, op_ref, *scratch):
    qa_ref, acc_ref, sum_ref, max_ref = scratch
    z, y, x, c = (lax.axis_index(n) for n in ("z", "y", "x", "c"))
    g = x // 2
    own = (4 * z + y) * 8 + 2 * x + c
    chunk = chunk_pieces * 128
    row8 = lax.broadcasted_iota(jnp.int32, (8, 128), 0)
    ones = jnp.where(row8 < 3, 1.0, 0.0).astype(f32)
    for rg, out_ref in enumerate((oo_ref, op_ref)):
        blk = own if rg == 0 else 127 - own
        dec = kvd_ref[blk, 128:160].astype(f32)
        dec = dec[0:8] + dec[8:16] + dec[16:24]
        ref_d = jnp.broadcast_to(dec[:, 0:1], (8, 128))
        parts = split3(dec - ref_d)
        for h in range(8):
            onehot = jnp.where(row8 == h, -1.0, 0.0).astype(f32)
            mine = jnp.zeros((8, 128), f32)
            for i, part in enumerate(parts):
                mine = jnp.where(row8 == i, part[h : h + 1], mine)
            rows = jnp.concatenate([onehot, onehot, onehot, mine], axis=0).astype(bf)
            if rg == 0:
                first = pl.multiple_of(g * 512 + h * 64, 64)
                query = q_ref[pl.ds(first, 64), :]
            else:
                query = part_ref[h * 64 : (h + 1) * 64, :]
            qa_ref[:, h * 128 : (h + 1) * 128] = jnp.concatenate(
                [query, rows, jnp.zeros((32, 128), bf)], axis=0
            )
        acc_ref[...] = jnp.zeros_like(acc_ref)
        sum_ref[...] = jnp.zeros_like(sum_ref)
        if not bounded:
            max_ref[...] = jnp.full(max_ref.shape, -1e30, f32)

        def attend_chunk(piece, masked):
            loaded = [load_keys(kvd_ref, piece + j, ref_d, ones) for j in range(chunk_pieces)]
            keys = jnp.concatenate([k for k, _ in loaded], axis=0)
            values = jnp.concatenate([v for _, v in loaded], axis=1)
            for n in range(1024 // tile):
                cols = slice(n * tile, (n + 1) * tile)
                scores = jnp.dot(keys, qa_ref[:, cols], preferred_element_type=f32)
                if masked:
                    shape = (chunk, tile)
                    key_pos = piece * 128 + lax.broadcasted_iota(jnp.int32, shape, 0)
                    query_pos = blk * 128 + (lax.broadcasted_iota(jnp.int32, shape, 1) & 127)
                    scores = jnp.where(key_pos <= query_pos, scores, -1e30)
                if bounded:
                    weights = jnp.exp2(scores)
                    sums = jnp.sum(weights.reshape(chunk // 8, 8, tile), axis=0)
                    sum_ref[:, cols] += sums
                    acc_ref[:, cols] += jnp.dot(
                        values, weights.astype(bf), preferred_element_type=f32
                    )
                else:
                    old = max_ref[0:1, cols]
                    new = jnp.maximum(old, jnp.max(scores, axis=0, keepdims=True))
                    keep = jnp.exp2(old - new)
                    weights = jnp.exp2(scores - new)
                    max_ref[:, cols] = jnp.broadcast_to(new, (8, tile))
                    sums = jnp.sum(weights.reshape(chunk // 8, 8, tile), axis=0)
                    sum_ref[:, cols] = sum_ref[:, cols] * keep + sums
                    acc_ref[:, cols] = acc_ref[:, cols] * keep + jnp.dot(
                        values, weights.astype(bf), preferred_element_type=f32
                    )

        full = blk // chunk_pieces

        def body(i, carry):
            attend_chunk(i * chunk_pieces, False)
            return carry

        lax.fori_loop(0, full, body, 0)
        attend_chunk(full * chunk_pieces, True)
        inverse = 1.0 / jnp.sum(sum_ref[...], axis=0, keepdims=True)
        for h in range(8):
            cols = slice(h * 128, (h + 1) * 128)
            out_ref[h * 64 : (h + 1) * 64, :] = (acc_ref[:, cols] * inverse[:, cols]).astype(bf)


def attend(q, part, kvd, bounded):
    chunk_pieces, tile = (8, 512) if bounded else (4, 256)
    return pl.pallas_call(
        functools.partial(attend_kernel, bounded, chunk_pieces, tile),
        out_shape=[jax.ShapeDtypeStruct((512, 128), bf)] * 2,
        in_specs=[VM, VM, VM],
        out_specs=[VM, VM],
        scratch_shapes=[
            pltpu.VMEM((128, 1024), bf),
            pltpu.VMEM((64, 1024), f32),
            pltpu.VMEM((8, 1024), f32),
            pltpu.VMEM((8, 1024), f32),
        ],
        compiler_params=pltpu.CompilerParams(vmem_limit_bytes=32 * 1024 * 1024),
        cost_estimate=pl.CostEstimate(
            flops=4 * 64 * 1024 * 17408, bytes_accessed=6 * 1024 * 1024, transcendentals=0
        ),
        name="attend_bounded" if bounded else "attend_any",
    )(q, part, kvd)


def output_kernel(oo_ref, op_ref, w_ref, out_ref, got_ref, send_sem, recv_sem):
    z, y, x, c = (lax.axis_index(n) for n in ("z", "y", "x", "c"))
    g = x // 2
    mirror = (3 - z, 3 - y, 3 - x, 1 - c)
    barrier = pltpu.get_barrier_semaphore()
    pl.semaphore_signal(barrier, inc=1, device_id=mirror, device_id_type=MESH)
    pl.semaphore_wait(barrier, 1)
    copy = pltpu.make_async_remote_copy(
        src_ref=op_ref,
        dst_ref=got_ref,
        send_sem=send_sem,
        recv_sem=recv_sem,
        device_id=mirror,
        device_id_type=MESH,
    )
    copy.start()
    here = oo_ref[...].T
    near = pl.multiple_of(g * 512, 512)
    far = pl.multiple_of((1 - g) * 512, 512)
    partial = jnp.dot(here, w_ref[pl.ds(near, 512), :], preferred_element_type=f32)
    copy.wait_recv()
    there = got_ref[...].T
    partial += jnp.dot(there, w_ref[pl.ds(far, 512), :], preferred_element_type=f32)
    out_ref[...] = partial.astype(bf)
    copy.wait_send()


def output(oo, op, w):
    return pl.pallas_call(
        output_kernel,
        out_shape=jax.ShapeDtypeStruct((128, 2048), bf),
        in_specs=[VM, VM, VM],
        out_specs=VM,
        scratch_shapes=[
            pltpu.VMEM((512, 128), bf),
            pltpu.SemaphoreType.DMA,
            pltpu.SemaphoreType.DMA,
        ],
        compiler_params=pltpu.CompilerParams(
            collective_id=1, has_side_effects=True, vmem_limit_bytes=24 * 1024 * 1024
        ),
        name="output",
    )(oo, op, w)


def per_device(inputs, in_gain, w_query, w_key, w_value, query_gain, key_gain, decay_sums, w_out):
    queries, kv = project(
        inputs,
        in_gain.reshape(1, -1),
        w_key,
        w_value,
        w_query,
        query_gain.reshape(-1, 1),
        key_gain.reshape(-1, 1),
    )
    part, kvd = gather(queries, kv, decay_sums.T)
    kvd = kvd.reshape(128, 160, 128)
    bound = 8.0 * 1.02 * jnp.max(jnp.abs(query_gain * key_gain))
    own_out, part_out = lax.cond(
        bound <= 64.0,
        lambda *a: attend(*a, True),
        lambda *a: attend(*a, False),
        queries,
        part,
        kvd,
    )
    return output(own_out, part_out, w_out)


def solution(mesh):
    torus = Mesh(mesh.devices.reshape(4, 4, 4, 2), ("z", "y", "x", "c"))
    every = ("z", "y", "x", "c")
    in_specs = (P(every, None), P(), P(), P(), P(), P(), P(), P(("z", "y"), ("x", "c")), P())
    return jax.shard_map(
        per_device, mesh=torus, in_specs=in_specs, out_specs=P(every, None), check_vma=False
    )
```

```python
import functools

import jax
import jax.numpy as jnp
from jax import lax
from jax.experimental import pallas as pl
from jax.experimental.pallas import tpu as pltpu
from jax.sharding import Mesh
from jax.sharding import PartitionSpec as P

f32 = jnp.float32
bf = jnp.bfloat16
LOG2E = 1.4426950408889634
EPS = 1e-06
MESH = pl.DeviceIdType.MESH
VM = pl.BlockSpec(memory_space=pltpu.VMEM)


def split3(x):
    high = x.astype(bf).astype(f32)
    rest = x - high
    mid = rest.astype(bf).astype(f32)
    return high, mid, rest - mid


def head_norm(flat, heads, gain):
    x = flat.reshape(heads, 64, flat.shape[1])
    scale = lax.rsqrt(jnp.mean(x * x, axis=1, keepdims=True) + EPS)
    return (x * scale * gain[None]).reshape(flat.shape)


HBM = pl.BlockSpec(memory_space=pltpu.HBM)
SEQ_J = (0, 3, 1, 0, 0, 2, 0, 3, 3, 1, 1, 3, 1, 2, 2, 2)
SEQ_K = (0, 0, 0, 3, 1, 0, 2, 3, 1, 3, 1, 2, 2, 3, 1, 2)


def column(row):
    return jnp.broadcast_to(row, (128, 64)).T


def start_kernel(x_hbm, gain_ref, wk_hbm, wv_hbm, qg_ref, kg_ref, norm_ref, kv_ref, bound_ref, *scratch):
    x_ref, wk_ref, wv_ref, sems = scratch
    copies = [
        pltpu.make_async_copy(src, dst, sems.at[i])
        for i, (src, dst) in enumerate(((x_hbm, x_ref), (wk_hbm, wk_ref), (wv_hbm, wv_ref)))
    ]
    for copy in copies:
        copy.start()
    bound_ref[0] = 8.0 * 1.02 * jnp.max(jnp.abs(qg_ref[...] * kg_ref[...]))
    gain = column(kg_ref[...])
    copies[0].wait()
    x = x_ref[...].astype(f32)
    scale = lax.rsqrt(jnp.mean(x * x, axis=1, keepdims=True) + EPS)
    norm_ref[...] = (x * scale * gain_ref[...]).astype(bf)
    copies[1].wait()
    keys = jnp.dot(norm_ref[...], wk_ref[...], preferred_element_type=f32)
    copies[2].wait()
    values = jnp.dot(norm_ref[...], wv_ref[...], preferred_element_type=f32)
    keys = head_norm(keys.T, 2, gain).astype(bf)
    values = values.T.astype(bf)
    for g in range(2):
        kv_ref[g, 0:64] = keys[g * 64 : (g + 1) * 64]
        kv_ref[g, 64:128] = values[g * 64 : (g + 1) * 64]


def start(x, gain, wk, wv, qg, kg):
    return pl.pallas_call(
        start_kernel,
        out_shape=[
            jax.ShapeDtypeStruct((128, 2048), bf),
            jax.ShapeDtypeStruct((2, 128, 128), bf),
            jax.ShapeDtypeStruct((1,), f32),
        ],
        in_specs=[HBM, VM, HBM, HBM, VM, VM],
        out_specs=[VM, VM, pl.BlockSpec(memory_space=pltpu.SMEM)],
        scratch_shapes=[
            pltpu.VMEM((128, 2048), bf),
            pltpu.VMEM((2048, 128), bf),
            pltpu.VMEM((2048, 128), bf),
            pltpu.SemaphoreType.DMA((3,)),
        ],
        compiler_params=pltpu.CompilerParams(vmem_limit_bytes=60 * 1024 * 1024),
        cost_estimate=pl.CostEstimate(
            flops=2 * 128 * 2048 * 256, bytes_accessed=2 * 1024 * 1024, transcendentals=0
        ),
        name="start",
    )(x, gain, wk, wv, qg, kg)


def load_keys(all_ref, line, p, ref_d, ones):
    dec = all_ref[line, p, 128:152].astype(f32)
    rel = dec[0:8] + dec[8:16] + dec[16:24] - ref_d
    rows = jnp.concatenate([*split3(rel), ones], axis=0).astype(bf)
    full = jnp.concatenate([all_ref[line, p, 0:64], rows, jnp.zeros((32, 128), bf)], axis=0)
    return full.T, all_ref[line, p, 64:128]


def main_kernel(bounded, tile, norm_ref, kv_ref, d_ref, qg_ref, wq_hbm, wo_hbm, out_ref, *scratch):
    all_ref, dec_ref, far_ref, wq_ref, wo_ref, part_ref = scratch[:6]
    qs_ref, qr_ref, os_ref, near_ref, got_ref = scratch[6:11]
    qa_ref, acc_ref, sum_ref, max_ref, refd_ref = scratch[11:16]
    w_sem, p_send, p_recv, d_send, d_recv, x_send, x_recv, r_send, r_recv, s_send, s_recv = scratch[16:]
    z, y, x, c = (lax.axis_index(n) for n in ("z", "y", "x", "c"))
    g = x // 2
    tp = 2 * x + c
    own_line = 4 * z + y
    mine = (x - 2 * g) * 2 + c
    mirror = (3 - z, 3 - y, 3 - x, 1 - c)
    across = (3 - z, 3 - y, x, c)
    sibling = (z, y, x, 1 - c)
    a = (1 - c) * y + c * z
    b = (1 - c) * z + c * y

    def line_at(j, k):
        pa, pb = lax.rem(a + j, 4), lax.rem(b + k, 4)
        return (1 - c) * (4 * pb + pa) + c * (4 * pa + pb)

    def at_ab(j, k):
        pa, pb = lax.rem(a + j, 4), lax.rem(b + k, 4)
        return ((1 - c) * pb + c * pa, (1 - c) * pa + c * pb, x, c)

    up_a, down_a, up_b, down_b = at_ab(1, 0), at_ab(3, 0), at_ab(0, 1), at_ab(0, 3)

    def remote(src, dst, send_sem, recv_sem, peer):
        return pltpu.make_async_remote_copy(
            src_ref=src,
            dst_ref=dst,
            send_sem=send_sem,
            recv_sem=recv_sem,
            device_id=peer,
            device_id_type=MESH,
        )

    w_far = pl.multiple_of((1 - g) * 512, 512)
    w_near = pl.multiple_of(g * 512, 512)
    far_copy = pltpu.make_async_copy(wq_hbm.at[:, pl.ds(w_far, 512)], wq_ref.at[0], w_sem.at[0])
    near_copy = pltpu.make_async_copy(wq_hbm.at[:, pl.ds(w_near, 512)], wq_ref.at[1], w_sem.at[1])
    out_copy = pltpu.make_async_copy(wo_hbm, wo_ref, w_sem.at[2])

    barrier = pltpu.get_barrier_semaphore()
    peers = [(z, y, lax.rem(x + k, 4), cc) for k in range(1, 4) for cc in range(2)]
    peers += [sibling, mirror, across, up_a, down_a, up_b, down_b]
    for peer in peers:
        pl.semaphore_signal(barrier, inc=1, device_id=peer, device_id_type=MESH)
    far_copy.start()
    near_copy.start()
    dec_ref[mine] = d_ref[...]

    @pl.when(g == c)
    def _():
        all_ref[own_line, tp, 0:128] = kv_ref[g]

    gain = column(qg_ref[...])
    pl.semaphore_wait(barrier, len(peers))

    def decay_copy(k):
        t = lax.rem(mine + k, 4)
        peer = (z, y, 2 * g + t // 2, lax.rem(t, 2))
        return remote(d_ref, dec_ref.at[mine], d_send.at[k], d_recv.at[k], peer)

    def piece_copy(k):
        to = lax.rem(x + k, 4)
        slot = (x - 2 * g) * 2 + c
        return remote(
            kv_ref.at[to // 2],
            all_ref.at[own_line, tp, pl.ds(0, 128)],
            p_send.at[k],
            p_recv.at[slot],
            (z, y, to, g),
        )

    for k in range(1, 4):
        decay_copy(k).start()
    for k in range(1, 4):
        piece_copy(k).start()

    @pl.when(g != c)
    def _():
        piece_copy(0).start()

    def queries(slot):
        flat = jnp.dot(norm_ref[...], wq_ref[slot], preferred_element_type=f32)
        return (head_norm(flat.T, 8, gain) * (LOG2E / 8)).astype(bf)

    far_copy.wait()
    qs_ref[...] = queries(0)

    for k in range(1, 4):
        decay_copy(k).wait_recv()
    for i in range(4):
        first = pl.multiple_of((4 * c + i) * 128, 128)
        value = jnp.concatenate([dec_ref[q, :, pl.ds(first, 128)] for q in range(4)], axis=0)
        all_ref[own_line, 4 * c + i, 128:152] = jnp.concatenate(
            split3(value * LOG2E), axis=0
        ).astype(bf)
    far_first = pl.multiple_of((7 - tp) * 128, 128)
    far_decays = remote(
        dec_ref.at[:, :, pl.ds(far_first, 128)], far_ref, x_send.at[0], x_recv.at[0], across
    )
    far_decays.start()
    q_copy = remote(qs_ref, qr_ref, x_send.at[1], x_recv.at[1], mirror)
    q_copy.start()

    def block(line, sub):
        return all_ref.at[line, pl.ds(4 * c + 2 * sub, 2)]

    def ring(step, slot):
        side = (0, 0, 0, 0, 3, 1)[slot]
        sub = (0, 1, 0, 1, 0, 1)[slot]
        upward = slot in (0, 1, 4)
        if step == 0:
            line, peer = line_at(side, 0), (up_a if upward else down_a)
        else:
            line, peer = line_at(step - 1, side), (up_b if upward else down_b)
        index = step * 6 + slot
        ref = block(line, sub)
        return remote(ref, ref, r_send.at[index], r_recv.at[index], peer)

    def share(j, k):
        half = all_ref.at[line_at(j, k), pl.ds(4 * c, 4)]
        index = j * 4 + k
        return remote(half, half, s_send.at[index], s_recv.at[index], sibling)

    def ring_start(step):
        for slot in range(4):
            ring(step, slot).start()

    def ring_relay(step):
        ring(step, 0).wait_recv()
        ring(step, 4).start()
        ring(step, 3).wait_recv()
        ring(step, 5).start()
        ring(step, 1).wait_recv()
        ring(step, 2).wait_recv()

    def ring_end(step):
        ring(step, 4).wait_recv()
        ring(step, 5).wait_recv()

    for i in range(4):

        @pl.when(4 * c + i != tp)
        def _():
            remote(
                kv_ref.at[0],
                all_ref.at[own_line, 4 * c + i, pl.ds(0, 128)],
                p_send.at[0],
                p_recv.at[i],
                sibling,
            ).wait_recv()

    ring_start(0)
    ring_start(1)
    share(0, 0).start()

    row8 = lax.broadcasted_iota(jnp.int32, (8, 128), 0)
    ones = jnp.where(row8 < 3, 1.0, 0.0).astype(f32)

    def prepare(rg, query_ref, decays):
        ref_d = jnp.broadcast_to(decays[:, 0:1], (8, 128))
        refd_ref[rg] = ref_d
        parts = split3(decays - ref_d)
        for h in range(8):
            onehot = jnp.where(row8 == h, -1.0, 0.0).astype(f32)
            own = jnp.zeros((8, 128), f32)
            for i, part in enumerate(parts):
                own = jnp.where(row8 == i, part[h : h + 1], own)
            rows = jnp.concatenate([onehot, onehot, onehot, own], axis=0).astype(bf)
            qa_ref[rg, :, h * 128 : (h + 1) * 128] = jnp.concatenate(
                [query_ref[h * 64 : (h + 1) * 64, :], rows, jnp.zeros((32, 128), bf)], axis=0
            )

    near_copy.wait()
    out_copy.start()
    near_ref[...] = queries(1)
    here = pl.multiple_of(tp * 128, 128)
    own_decays = jnp.concatenate([dec_ref[q, :, pl.ds(here, 128)] for q in range(4)], axis=0)
    prepare(0, near_ref, own_decays * LOG2E)
    acc_ref[...] = jnp.zeros_like(acc_ref)
    sum_ref[...] = jnp.zeros_like(sum_ref)
    if not bounded:
        max_ref[...] = jnp.full(max_ref.shape, -1e30, f32)

    def attend(rg, line, tp_row, masked):
        ref_d = refd_ref[rg]
        loaded = [load_keys(all_ref, line, p, ref_d, ones) for p in range(8)]
        keys = jnp.concatenate([k for k, _ in loaded], axis=0)
        values = jnp.concatenate([v for _, v in loaded], axis=1)
        for n in range(1024 // tile):
            cols = slice(n * tile, (n + 1) * tile)
            scores = jnp.dot(keys, qa_ref[rg, :, cols], preferred_element_type=f32)
            if masked:
                key_pos = lax.broadcasted_iota(jnp.int32, (1024, tile), 0)
                query_pos = tp_row * 128 + (lax.broadcasted_iota(jnp.int32, (1024, tile), 1) & 127)
                scores = jnp.where(key_pos <= query_pos, scores, -1e30)
            if bounded:
                weights = jnp.exp2(scores)
                sum_ref[rg, :, cols] += jnp.sum(weights.reshape(128, 8, tile), axis=0)
                acc_ref[rg, :, cols] += jnp.dot(
                    values, weights.astype(bf), preferred_element_type=f32
                )
            else:
                old = max_ref[rg, 0:1, cols]
                new = jnp.maximum(old, jnp.max(scores, axis=0, keepdims=True))
                keep = jnp.exp2(old - new)
                weights = jnp.exp2(scores - new)
                max_ref[rg, :, cols] = jnp.broadcast_to(new, (8, tile))
                sums = jnp.sum(weights.reshape(128, 8, tile), axis=0)
                sum_ref[rg, :, cols] = sum_ref[rg, :, cols] * keep + sums
                acc_ref[rg, :, cols] = acc_ref[rg, :, cols] * keep + jnp.dot(
                    values, weights.astype(bf), preferred_element_type=f32
                )

    def act_1():
        ring_relay(0)
        share(3, 0).start()
        share(1, 0).start()
        ring_relay(1)
        ring_start(4)
        ring_start(2)
        share(0, 3).start()
        share(0, 1).start()

    def act_3():
        ring_end(0)
        ring_start(3)
        share(2, 0).start()
        ring_end(1)
        share(0, 2).start()

    def act_6():
        for j in (3, 1):
            ring_relay(1 + j)
            share(j, 3).start()
            share(j, 1).start()

    def act_9():
        ring_relay(3)
        share(2, 3).start()
        share(2, 1).start()
        for j in (3, 1):
            ring_end(1 + j)
            share(j, 2).start()

    def act_13():
        ring_end(3)
        share(2, 2).start()

    actions = {1: act_1, 3: act_3, 6: act_6, 9: act_9, 13: act_13}

    def table(values, step):
        total = 0
        for i, value in enumerate(values):
            if value:
                total = total + value * (step == i).astype(jnp.int32)
        return total

    def body(step, carry):
        for at, action in actions.items():

            @pl.when(step == at)
            def _(action=action):
                action()

        j, k = table(SEQ_J, step), table(SEQ_K, step)
        line = line_at(j, k)
        index = k * 4 + j
        half = all_ref.at[line, pl.ds(4 * (1 - c), 4)]
        remote(half, half, s_send.at[index], s_recv.at[index], sibling).wait_recv()

        def group(rg, inner):
            @pl.when((step == 0) & (rg == 1))
            def _():
                far_decays.wait_recv()
                q_copy.wait_recv()
                far = jnp.concatenate([far_ref[q] for q in range(4)], axis=0)
                prepare(1, qr_ref, far * LOG2E)

            last = own_line + rg * (15 - 2 * own_line)
            tp_row = tp + rg * (7 - 2 * tp)

            @pl.when(line < last)
            def _():
                attend(rg, line, tp_row, False)

            @pl.when(line == last)
            def _():
                attend(rg, line, tp_row, True)

            return inner

        return lax.fori_loop(0, 2, group, carry)

    lax.fori_loop(0, 16, body, 0)

    def finish(rg, to_ref):
        inverse = 1.0 / jnp.sum(sum_ref[rg], axis=0, keepdims=True)
        for h in range(8):
            cols = slice(h * 128, (h + 1) * 128)
            to_ref[h * 64 : (h + 1) * 64, :] = (acc_ref[rg, :, cols] * inverse[:, cols]).astype(bf)

    finish(1, os_ref)
    finish(0, near_ref)
    back = remote(os_ref, got_ref, x_send.at[2], x_recv.at[2], mirror)
    back.start()
    out_copy.wait()
    near = near_ref[...].T
    for n in range(4):
        cols = slice(n * 512, (n + 1) * 512)
        part_ref[:, cols] = jnp.dot(near, wo_ref[pl.ds(w_near, 512), cols], preferred_element_type=f32)
    for k in range(1, 4):
        decay_copy(k).wait_send()
        piece_copy(k).wait_send()

    @pl.when(g != c)
    def _():
        piece_copy(0).wait_send()

    far_decays.wait_send()
    q_copy.wait_send()
    for step in range(5):
        for slot in range(6):
            ring(step, slot).wait_send()
    for j in range(4):
        for k in range(4):
            share(j, k).wait_send()
    back.wait_recv()
    far = got_ref[...].T
    for n in range(4):
        cols = slice(n * 512, (n + 1) * 512)
        rest = jnp.dot(far, wo_ref[pl.ds(w_far, 512), cols], preferred_element_type=f32)
        out_ref[:, cols] = (part_ref[:, cols] + rest).astype(bf)
    back.wait_send()


def main(norm, kv, d, qg, wq, wo, bounded):
    dma = lambda *n: pltpu.SemaphoreType.DMA(n)
    return pl.pallas_call(
        functools.partial(main_kernel, bounded, 512 if bounded else 256),
        out_shape=jax.ShapeDtypeStruct((128, 2048), bf),
        in_specs=[VM, VM, VM, VM, HBM, HBM],
        out_specs=VM,
        scratch_shapes=[
            pltpu.VMEM((16, 8, 152, 128), bf),
            pltpu.VMEM((4, 2, 1024), f32),
            pltpu.VMEM((4, 2, 128), f32),
            pltpu.VMEM((2, 2048, 512), bf),
            pltpu.VMEM((1024, 2048), bf),
            pltpu.VMEM((128, 2048), f32),
            pltpu.VMEM((512, 128), bf),
            pltpu.VMEM((512, 128), bf),
            pltpu.VMEM((512, 128), bf),
            pltpu.VMEM((512, 128), bf),
            pltpu.VMEM((512, 128), bf),
            pltpu.VMEM((2, 128, 1024), bf),
            pltpu.VMEM((2, 64, 1024), f32),
            pltpu.VMEM((2, 8, 1024), f32),
            pltpu.VMEM((2, 8, 1024), f32),
            pltpu.VMEM((2, 8, 128), f32),
            dma(3),
            dma(4),
            dma(4),
            dma(4),
            dma(4),
            dma(3),
            dma(3),
            dma(30),
            dma(30),
            dma(16),
            dma(16),
        ],
        compiler_params=pltpu.CompilerParams(
            collective_id=0 if bounded else 1,
            has_side_effects=True,
            vmem_limit_bytes=60 * 1024 * 1024,
        ),
        name="main_bounded" if bounded else "main_any",
    )(norm, kv, d, qg, wq, wo)


def per_device(inputs, in_gain, w_query, w_key, w_value, query_gain, key_gain, decay_sums, w_out):
    query_gain = query_gain.reshape(1, -1)
    key_gain = key_gain.reshape(1, -1)
    norm, kv, bound = start(inputs, in_gain.reshape(1, -1), w_key, w_value, query_gain, key_gain)
    return lax.cond(
        bound[0] <= 64.0,
        lambda *a: main(*a, True),
        lambda *a: main(*a, False),
        norm,
        kv,
        decay_sums.T,
        query_gain,
        w_query,
        w_out,
    )


def solution(mesh):
    torus = Mesh(mesh.devices.reshape(4, 4, 4, 2), ("z", "y", "x", "c"))
    every = ("z", "y", "x", "c")
    in_specs = (P(every, None), P(), P(), P(), P(), P(), P(), P(("z", "y"), ("x", "c")), P())
    return jax.shard_map(
        per_device, mesh=torus, in_specs=in_specs, out_specs=P(every, None), check_vma=False
    )
```

```python
import functools

import jax
import jax.numpy as jnp
from jax import lax
from jax.experimental import pallas as pl
from jax.experimental.pallas import tpu as pltpu
from jax.sharding import Mesh
from jax.sharding import PartitionSpec as P

f32 = jnp.float32
bf = jnp.bfloat16
LOG2E = 1.4426950408889634
EPS = 1e-06
MESH = pl.DeviceIdType.MESH
VM = pl.BlockSpec(memory_space=pltpu.VMEM)


def split3(x):
    high = x.astype(bf).astype(f32)
    rest = x - high
    mid = rest.astype(bf).astype(f32)
    return high, mid, rest - mid


def head_norm(flat, heads, gain):
    x = flat.reshape(heads, 64, flat.shape[1])
    scale = lax.rsqrt(jnp.mean(x * x, axis=1, keepdims=True) + EPS)
    return (x * scale * gain[None]).reshape(flat.shape)


HBM = pl.BlockSpec(memory_space=pltpu.HBM)
SEQ_J = (0, 3, 1, 0, 0, 2, 0, 3, 3, 1, 1, 3, 1, 2, 2, 2)
SEQ_K = (0, 0, 0, 3, 1, 0, 2, 3, 1, 3, 1, 2, 2, 3, 1, 2)
ROWS, LAG = 256, 3


def packed(values):
    total = sum(v << 2 * i for i, v in enumerate(values))
    return total - (1 << 32) if total >> 31 else total


def unpacked(values, index):
    return lax.shift_right_logical(jnp.int32(packed(values)), 2 * index) & 3


def column(row):
    return jnp.broadcast_to(row, (128, 64)).T


def load_keys(all_ref, line, p, ref_d, ones):
    dec = all_ref[line, p, 128:152].astype(f32)
    rel = dec[0:8] + dec[8:16] + dec[16:24] - ref_d
    rows = jnp.concatenate([*split3(rel), ones], axis=0).astype(bf)
    full = jnp.concatenate([all_ref[line, p, 0:64], rows, jnp.zeros((32, 128), bf)], axis=0)
    return full.T


def main_kernel(bounded, tile, *refs):
    x_hbm, in_gain_ref, wk_hbm, wv_hbm, qg_ref, kg_ref, d_ref, wq_hbm, wo_hbm = refs[:9]
    out_ref, bound_ref = refs[9:11]
    x_ref, wk_ref, wv_ref, norm_ref, kv_ref = refs[11:16]
    scratch = refs[16:]
    all_ref, dec_ref, far_ref, wq_ref, wo_ref, part_ref = scratch[:6]
    qs_ref, qr_ref, os_ref, near_ref, got_ref = scratch[6:11]
    qa_ref, acc_ref, sum_ref, max_ref, refd_ref, ka_ref, wt_ref = scratch[11:18]
    w_sem, p_send, p_recv, d_send, d_recv, x_send, x_recv, r_send, r_recv, s_send, s_recv = scratch[18:]
    z, y, x, c = (lax.axis_index(n) for n in ("z", "y", "x", "c"))
    g = x // 2
    tp = 2 * x + c
    own_line = 4 * z + y
    mine = (x - 2 * g) * 2 + c
    mirror = (3 - z, 3 - y, 3 - x, 1 - c)
    across = (3 - z, 3 - y, x, c)
    sibling = (z, y, x, 1 - c)
    a = (1 - c) * y + c * z
    b = (1 - c) * z + c * y

    def line_at(j, k):
        pa, pb = (a + j) & 3, (b + k) & 3
        return (1 - c) * (4 * pb + pa) + c * (4 * pa + pb)

    def at_ab(j, k):
        pa, pb = (a + j) & 3, (b + k) & 3
        return ((1 - c) * pb + c * pa, (1 - c) * pa + c * pb, x, c)

    up_a, down_a, up_b, down_b = at_ab(1, 0), at_ab(3, 0), at_ab(0, 1), at_ab(0, 3)

    def remote(src, dst, send_sem, recv_sem, peer):
        return pltpu.make_async_remote_copy(
            src_ref=src,
            dst_ref=dst,
            send_sem=send_sem,
            recv_sem=recv_sem,
            device_id=peer,
            device_id_type=MESH,
        )

    w_far = pl.multiple_of((1 - g) * 512, 512)
    w_near = pl.multiple_of(g * 512, 512)
    far_copy = pltpu.make_async_copy(wq_hbm.at[:, pl.ds(w_far, 512)], wq_ref.at[0], w_sem.at[0])
    near_copy = pltpu.make_async_copy(wq_hbm.at[:, pl.ds(w_near, 512)], wq_ref.at[1], w_sem.at[1])
    out_copy = pltpu.make_async_copy(wo_hbm, wo_ref, w_sem.at[2])

    first_copies = [
        pltpu.make_async_copy(src, dst, w_sem.at[3 + i])
        for i, (src, dst) in enumerate(((x_hbm, x_ref), (wk_hbm, wk_ref), (wv_hbm, wv_ref)))
    ]
    for copy in first_copies:
        copy.start()
    barrier = pltpu.get_barrier_semaphore()
    peers = [(z, y, lax.rem(x + k, 4), cc) for k in range(1, 4) for cc in range(2)]
    peers += [sibling, mirror, across, up_a, down_a, up_b, down_b]
    for peer in peers:
        pl.semaphore_signal(barrier, inc=1, device_id=peer, device_id_type=MESH)
    far_copy.start()
    near_copy.start()
    dec_ref[mine] = d_ref[...]
    bound_ref[0] = 8.0 * 1.02 * jnp.max(jnp.abs(qg_ref[...] * kg_ref[...]))
    gain = column(qg_ref[...])
    key_gain = column(kg_ref[...])

    first_copies[0].wait()
    rows = x_ref[...].astype(f32)
    scale = lax.rsqrt(jnp.mean(rows * rows, axis=1, keepdims=True) + EPS)
    norm_ref[...] = (rows * scale * in_gain_ref[...]).astype(bf)
    first_copies[1].wait()
    keys = jnp.dot(norm_ref[...], wk_ref[...], preferred_element_type=f32)
    first_copies[2].wait()
    values = jnp.dot(norm_ref[...], wv_ref[...], preferred_element_type=f32)
    keys = head_norm(keys.T, 2, key_gain).astype(bf)
    values = values.T.astype(bf)
    for i in range(2):
        kv_ref[i, 0:64] = keys[i * 64 : (i + 1) * 64]
        kv_ref[i, 64:128] = values[i * 64 : (i + 1) * 64]

    @pl.when(g == c)
    def _():
        all_ref[own_line, tp, 0:128] = kv_ref[g]

    pl.semaphore_wait(barrier, len(peers))

    def decay_copy(k):
        t = lax.rem(mine + k, 4)
        peer = (z, y, 2 * g + t // 2, lax.rem(t, 2))
        return remote(d_ref, dec_ref.at[mine], d_send.at[k], d_recv.at[k], peer)

    def piece_copy(k):
        to = lax.rem(x + k, 4)
        slot = (x - 2 * g) * 2 + c
        return remote(
            kv_ref.at[to // 2],
            all_ref.at[own_line, tp, pl.ds(0, 128)],
            p_send.at[k],
            p_recv.at[slot],
            (z, y, to, g),
        )

    for k in range(1, 4):
        decay_copy(k).start()
    for k in range(1, 4):
        piece_copy(k).start()

    @pl.when(g != c)
    def _():
        piece_copy(0).start()

    def queries(slot):
        flat = jnp.dot(norm_ref[...], wq_ref[slot], preferred_element_type=f32)
        return (head_norm(flat.T, 8, gain) * (LOG2E / 8)).astype(bf)

    far_copy.wait()
    qs_ref[...] = queries(0)

    for k in range(1, 4):
        decay_copy(k).wait_recv()
    for i in range(4):
        first = pl.multiple_of((4 * c + i) * 128, 128)
        value = jnp.concatenate([dec_ref[q, :, pl.ds(first, 128)] for q in range(4)], axis=0)
        all_ref[own_line, 4 * c + i, 128:152] = jnp.concatenate(
            split3(value * LOG2E), axis=0
        ).astype(bf)
    far_first = pl.multiple_of((7 - tp) * 128, 128)
    far_decays = remote(
        dec_ref.at[:, :, pl.ds(far_first, 128)], far_ref, x_send.at[0], x_recv.at[0], across
    )
    far_decays.start()
    q_copy = remote(qs_ref, qr_ref, x_send.at[1], x_recv.at[1], mirror)
    late = own_line < 8

    @pl.when(jnp.logical_not(late))
    def _():
        q_copy.start()

    def block(line, sub):
        return all_ref.at[line, pl.ds(4 * c + 2 * sub, 2)]

    def ring(step, slot):
        side = (0, 0, 0, 0, 3, 1)[slot]
        sub = (0, 1, 0, 1, 0, 1)[slot]
        upward = slot in (0, 1, 4)
        if step == 0:
            line, peer = line_at(side, 0), (up_a if upward else down_a)
        else:
            line, peer = line_at(step - 1, side), (up_b if upward else down_b)
        index = step * 6 + slot
        ref = block(line, sub)
        return remote(ref, ref, r_send.at[index], r_recv.at[index], peer)

    def share(j, k):
        half = all_ref.at[line_at(j, k), pl.ds(4 * c, 4)]
        index = j * 4 + k
        return remote(half, half, s_send.at[index], s_recv.at[index], sibling)

    def ring_start(step):
        for slot in range(4):
            ring(step, slot).start()

    def ring_relay(step):
        ring(step, 0).wait_recv()
        ring(step, 4).start()
        ring(step, 3).wait_recv()
        ring(step, 5).start()
        ring(step, 1).wait_recv()
        ring(step, 2).wait_recv()

    def ring_end(step):
        ring(step, 4).wait_recv()
        ring(step, 5).wait_recv()

    for i in range(4):

        @pl.when(4 * c + i != tp)
        def _():
            remote(
                kv_ref.at[0],
                all_ref.at[own_line, 4 * c + i, pl.ds(0, 128)],
                p_send.at[0],
                p_recv.at[i],
                sibling,
            ).wait_recv()

    ring_start(0)
    ring_start(1)
    share(0, 0).start()

    row8 = lax.broadcasted_iota(jnp.int32, (8, 128), 0)
    ones = jnp.where(row8 < 3, 1.0, 0.0).astype(f32)

    def prepare(rg, query_ref, decays):
        ref_d = jnp.broadcast_to(decays[:, 0:1], (8, 128))
        refd_ref[rg] = ref_d
        parts = split3(decays - ref_d)
        for h in range(8):
            onehot = jnp.where(row8 == h, -1.0, 0.0).astype(f32)
            own = jnp.zeros((8, 128), f32)
            for i, part in enumerate(parts):
                own = jnp.where(row8 == i, part[h : h + 1], own)
            rows = jnp.concatenate([onehot, onehot, onehot, own], axis=0).astype(bf)
            qa_ref[rg, :, h * 128 : (h + 1) * 128] = jnp.concatenate(
                [query_ref[h * 64 : (h + 1) * 64, :], rows, jnp.zeros((32, 128), bf)], axis=0
            )

    near_copy.wait()
    out_copy.start()
    near_ref[...] = queries(1)
    here = pl.multiple_of(tp * 128, 128)
    own_decays = jnp.concatenate([dec_ref[q, :, pl.ds(here, 128)] for q in range(4)], axis=0)
    prepare(0, near_ref, own_decays * LOG2E)
    acc_ref[...] = jnp.zeros_like(acc_ref)
    sum_ref[...] = jnp.zeros_like(sum_ref)
    if not bounded:
        max_ref[...] = jnp.full(max_ref.shape, -1e30, f32)

    def attend(rg, line, tp_row, masked):
        ref_d = refd_ref[rg]
        for p in range(8):
            ka_ref[p * 128 : (p + 1) * 128] = load_keys(all_ref, line, p, ref_d, ones)
        units = [(m, n) for m in range(1024 // ROWS) for n in range(1024 // tile)]

        def weigh(u):
            m, n = units[u]
            cols = slice(n * tile, (n + 1) * tile)
            keys = ka_ref[m * ROWS : (m + 1) * ROWS]
            scores = jnp.dot(keys, qa_ref[rg, :, cols], preferred_element_type=f32)
            if masked:
                shape = (ROWS, tile)
                key_pos = m * ROWS + lax.broadcasted_iota(jnp.int32, shape, 0)
                query_pos = tp_row * 128 + (lax.broadcasted_iota(jnp.int32, shape, 1) & 127)
                scores = jnp.where(key_pos <= query_pos, scores, -1e30)
            if bounded:
                weights = jnp.exp2(scores)
                sum_ref[rg, :, cols] += jnp.sum(weights.reshape(ROWS // 8, 8, tile), axis=0)
            else:
                old = max_ref[rg, 0:1, cols]
                new = jnp.maximum(old, jnp.max(scores, axis=0, keepdims=True))
                keep = jnp.exp2(old - new)
                weights = jnp.exp2(scores - new)
                max_ref[rg, :, cols] = jnp.broadcast_to(new, (8, tile))
                sums = jnp.sum(weights.reshape(ROWS // 8, 8, tile), axis=0)
                sum_ref[rg, :, cols] = sum_ref[rg, :, cols] * keep + sums
                acc_ref[rg, :, cols] = acc_ref[rg, :, cols] * keep
            wt_ref[u % (lag + 1)] = weights.astype(bf)

        def gather_values(u):
            m, n = units[u]
            cols = slice(n * tile, (n + 1) * tile)
            first = m * ROWS // 128
            values = jnp.concatenate(
                [all_ref[line, p, 64:128] for p in range(first, first + ROWS // 128)], axis=1
            )
            acc_ref[rg, :, cols] += jnp.dot(
                values, wt_ref[u % (lag + 1)], preferred_element_type=f32
            )

        lag = LAG if bounded else 0
        for u in range(len(units) + lag):
            if u < len(units):
                weigh(u)
            if u >= lag:
                gather_values(u - lag)

    def act_1():
        ring_relay(0)
        share(3, 0).start()
        share(1, 0).start()
        ring_relay(1)

        @pl.when(late)
        def _():
            q_copy.start()

        ring_start(4)
        ring_start(2)
        share(0, 3).start()
        share(0, 1).start()

    def act_3():
        ring_end(0)
        ring_start(3)
        share(2, 0).start()
        ring_end(1)
        share(0, 2).start()

    def act_6():
        for j in (3, 1):
            ring_relay(1 + j)
            share(j, 3).start()
            share(j, 1).start()

    def act_9():
        ring_relay(3)
        share(2, 3).start()
        share(2, 1).start()
        for j in (3, 1):
            ring_end(1 + j)
            share(j, 2).start()

    def act_13():
        ring_end(3)
        share(2, 2).start()

    actions = {1: act_1, 4: act_3, 7: act_6, 10: act_9, 14: act_13}

    later = jnp.where(late, 0, 1)

    def body(step, carry):
        for at, action in actions.items():

            @pl.when(step == at)
            def _(action=action):
                action()

        place = jnp.maximum(step - 1, 0) & 15
        j, k = unpacked(SEQ_J, place), unpacked(SEQ_K, place)
        again = (step >= 17).astype(jnp.int32)
        line = line_at(j, k) * (1 - again) + (step - 17) * again

        @pl.when((step != 1) & (step < 17))
        def _():
            index = k * 4 + j
            half = all_ref.at[line, pl.ds(4 * (1 - c), 4)]
            remote(half, half, s_send.at[index], s_recv.at[index], sibling).wait_recv()

        @pl.when(step == 1 + 16 * later)
        def _():
            far_decays.wait_recv()
            q_copy.wait_recv()
            far = jnp.concatenate([far_ref[q] for q in range(4)], axis=0)
            prepare(1, qr_ref, far * LOG2E)

        def group(rg, inner):
            last = own_line + rg * (15 - 2 * own_line)
            tp_row = tp + rg * (7 - 2 * tp)

            @pl.when(line < last)
            def _():
                attend(rg, line, tp_row, False)

            @pl.when(line == last)
            def _():
                attend(rg, line, tp_row, True)

            return inner

        one = lambda test: test.astype(jnp.int32)
        own_rows = one(line <= own_line) * one(step != 1) * (1 - again)
        far_rows = one(line <= 15 - own_line) * ((1 - later) * one(step != 0) + again)
        return lax.fori_loop(1 - own_rows, 1 + far_rows, group, carry)

    lax.fori_loop(0, 17 + later * (16 - own_line), body, 0)

    def finish(rg, to_ref):
        inverse = 1.0 / jnp.sum(sum_ref[rg], axis=0, keepdims=True)
        for h in range(8):
            cols = slice(h * 128, (h + 1) * 128)
            to_ref[h * 64 : (h + 1) * 64, :] = (acc_ref[rg, :, cols] * inverse[:, cols]).astype(bf)

    finish(1, os_ref)
    finish(0, near_ref)
    back = remote(os_ref, got_ref, x_send.at[2], x_recv.at[2], mirror)
    back.start()
    out_copy.wait()
    near = near_ref[...].T
    for n in range(4):
        cols = slice(n * 512, (n + 1) * 512)
        part_ref[:, cols] = jnp.dot(near, wo_ref[pl.ds(w_near, 512), cols], preferred_element_type=f32)
    for k in range(1, 4):
        decay_copy(k).wait_send()
        piece_copy(k).wait_send()

    @pl.when(g != c)
    def _():
        piece_copy(0).wait_send()

    far_decays.wait_send()
    q_copy.wait_send()
    for step in range(5):
        for slot in range(6):
            ring(step, slot).wait_send()
    for j in range(4):
        for k in range(4):
            share(j, k).wait_send()
    back.wait_recv()
    far = got_ref[...].T
    for n in range(4):
        cols = slice(n * 512, (n + 1) * 512)
        rest = jnp.dot(far, wo_ref[pl.ds(w_far, 512), cols], preferred_element_type=f32)
        out_ref[:, cols] = (part_ref[:, cols] + rest).astype(bf)
    back.wait_send()


def main(x, in_gain, wk, wv, qg, kg, d, wq, wo, bounded):
    dma = lambda *n: pltpu.SemaphoreType.DMA(n)
    return pl.pallas_call(
        functools.partial(main_kernel, bounded, 512),
        out_shape=[jax.ShapeDtypeStruct((128, 2048), bf), jax.ShapeDtypeStruct((1,), f32)],
        in_specs=[HBM, VM, HBM, HBM, VM, VM, VM, HBM, HBM],
        out_specs=[VM, pl.BlockSpec(memory_space=pltpu.SMEM)],
        scratch_shapes=[
            pltpu.VMEM((128, 2048), bf),
            pltpu.VMEM((2048, 128), bf),
            pltpu.VMEM((2048, 128), bf),
            pltpu.VMEM((128, 2048), bf),
            pltpu.VMEM((2, 128, 128), bf),
            pltpu.VMEM((16, 8, 152, 128), bf),
            pltpu.VMEM((4, 2, 1024), f32),
            pltpu.VMEM((4, 2, 128), f32),
            pltpu.VMEM((2, 2048, 512), bf),
            pltpu.VMEM((1024, 2048), bf),
            pltpu.VMEM((128, 2048), f32),
            pltpu.VMEM((512, 128), bf),
            pltpu.VMEM((512, 128), bf),
            pltpu.VMEM((512, 128), bf),
            pltpu.VMEM((512, 128), bf),
            pltpu.VMEM((512, 128), bf),
            pltpu.VMEM((2, 128, 1024), bf),
            pltpu.VMEM((2, 64, 1024), f32),
            pltpu.VMEM((2, 8, 1024), f32),
            pltpu.VMEM((2, 8, 1024), f32),
            pltpu.VMEM((2, 8, 128), f32),
            pltpu.VMEM((1024, 128), bf),
            pltpu.VMEM((LAG + 1, ROWS, 512), bf),
            dma(6),
            dma(4),
            dma(4),
            dma(4),
            dma(4),
            dma(3),
            dma(3),
            dma(30),
            dma(30),
            dma(16),
            dma(16),
        ],
        compiler_params=pltpu.CompilerParams(
            collective_id=0 if bounded else 1,
            has_side_effects=True,
            vmem_limit_bytes=67_000_000,
        ),
        name="main_bounded" if bounded else "main_any",
    )(x, in_gain, wk, wv, qg, kg, d, wq, wo)


def per_device(inputs, in_gain, w_query, w_key, w_value, query_gain, key_gain, decay_sums, w_out):
    args = (
        inputs,
        in_gain.reshape(1, -1),
        w_key,
        w_value,
        query_gain.reshape(1, -1),
        key_gain.reshape(1, -1),
        decay_sums.T,
        w_query,
        w_out,
    )
    result, bound = main(*args, True)
    return lax.cond(
        bound[0] <= 64.0, lambda kept, *a: kept, lambda kept, *a: main(*a, False)[0], result, *args
    )


def solution(mesh):
    torus = Mesh(mesh.devices.reshape(4, 4, 4, 2), ("z", "y", "x", "c"))
    every = ("z", "y", "x", "c")
    in_specs = (P(every, None), P(), P(), P(), P(), P(), P(), P(("z", "y"), ("x", "c")), P())
    return jax.shard_map(
        per_device, mesh=torus, in_specs=in_specs, out_specs=P(every, None), check_vma=False
    )
```

```python
import functools

import jax
import jax.numpy as jnp
from jax import lax
from jax.experimental import pallas as pl
from jax.experimental.pallas import tpu as pltpu
from jax.sharding import Mesh
from jax.sharding import PartitionSpec as P

f32 = jnp.float32
bf = jnp.bfloat16
LOG2E = 1.4426950408889634
EPS = 1e-06
MESH = pl.DeviceIdType.MESH
VM = pl.BlockSpec(memory_space=pltpu.VMEM)


def split3(x):
    high = x.astype(bf).astype(f32)
    rest = x - high
    mid = rest.astype(bf).astype(f32)
    return high, mid, rest - mid


def head_norm(flat, heads, gain):
    x = flat.reshape(heads, 64, flat.shape[1])
    scale = lax.rsqrt(jnp.mean(x * x, axis=1, keepdims=True) + EPS)
    return (x * scale * gain[None]).reshape(flat.shape)


HBM = pl.BlockSpec(memory_space=pltpu.HBM)
GROUPS = (
    ((0, 0), (3, 0), (0, 3)),
    ((1, 0), (0, 1)),
    ((2, 0), (0, 2)),
    ((3, 3), (1, 3)),
    ((3, 1), (1, 1)),
    ((3, 2), (1, 2), (2, 3), (2, 1)),
    ((2, 2),),
)
ROWS, LAG = 256, 3


def packed(values):
    total = sum(v << 4 * i for i, v in enumerate(values))
    return total - (1 << 32) if total >> 31 else total


def unpacked(values, index):
    return lax.shift_right_logical(jnp.int32(packed(values)), 4 * index) & 15


def column(row):
    return jnp.broadcast_to(row, (128, 64)).T


def load_keys(all_ref, line, p, ref_d, ones):
    dec = all_ref[line, p, 128:152].astype(f32)
    rel = dec[0:8] + dec[8:16] + dec[16:24] - ref_d
    rows = jnp.concatenate([*split3(rel), ones], axis=0).astype(bf)
    full = jnp.concatenate([all_ref[line, p, 0:64], rows, jnp.zeros((32, 128), bf)], axis=0)
    return full.T


def main_kernel(bounded, tile, *refs):
    x_hbm, in_gain_ref, wk_hbm, wv_hbm, qg_ref, kg_ref, d_ref, wq_hbm, wo_hbm = refs[:9]
    out_ref, bound_ref = refs[9:11]
    x_ref, wk_ref, wv_ref, norm_ref, kv_ref = refs[11:16]
    scratch = refs[16:]
    all_ref, dec_ref, far_ref, wq_ref, wo_ref, part_ref = scratch[:6]
    qs_ref, qr_ref, os_ref, near_ref, got_ref = scratch[6:11]
    qa_ref, acc_ref, sum_ref, max_ref, refd_ref, ka_ref, wt_ref = scratch[11:18]
    w_sem, p_send, p_recv, d_send, d_recv, x_send, x_recv, r_send, r_recv, s_send, s_recv = scratch[18:]
    z, y, x, c = (lax.axis_index(n) for n in ("z", "y", "x", "c"))
    g = x // 2
    tp = 2 * x + c
    own_line = 4 * z + y
    mine = (x - 2 * g) * 2 + c
    mirror = (3 - z, 3 - y, 3 - x, 1 - c)
    across = (3 - z, 3 - y, x, c)
    sibling = (z, y, x, 1 - c)
    a = (1 - c) * y + c * z
    b = (1 - c) * z + c * y

    def line_at(j, k):
        pa, pb = (a + j) & 3, (b + k) & 3
        return (1 - c) * (4 * pb + pa) + c * (4 * pa + pb)

    def at_ab(j, k):
        pa, pb = (a + j) & 3, (b + k) & 3
        return ((1 - c) * pb + c * pa, (1 - c) * pa + c * pb, x, c)

    up_a, down_a, up_b, down_b = at_ab(1, 0), at_ab(3, 0), at_ab(0, 1), at_ab(0, 3)

    def remote(src, dst, send_sem, recv_sem, peer):
        return pltpu.make_async_remote_copy(
            src_ref=src,
            dst_ref=dst,
            send_sem=send_sem,
            recv_sem=recv_sem,
            device_id=peer,
            device_id_type=MESH,
        )

    w_far = pl.multiple_of((1 - g) * 512, 512)
    w_near = pl.multiple_of(g * 512, 512)
    far_copy = pltpu.make_async_copy(wq_hbm.at[:, pl.ds(w_far, 512)], wq_ref.at[0], w_sem.at[0])
    near_copy = pltpu.make_async_copy(wq_hbm.at[:, pl.ds(w_near, 512)], wq_ref.at[1], w_sem.at[1])
    out_copy = pltpu.make_async_copy(wo_hbm, wo_ref, w_sem.at[2])

    first_copies = [
        pltpu.make_async_copy(src, dst, w_sem.at[3 + i])
        for i, (src, dst) in enumerate(((x_hbm, x_ref), (wk_hbm, wk_ref), (wv_hbm, wv_ref)))
    ]
    for copy in first_copies:
        copy.start()
    barrier = pltpu.get_barrier_semaphore()
    peers = [(z, y, lax.rem(x + k, 4), cc) for k in range(1, 4) for cc in range(2)]
    peers += [sibling, mirror, across, up_a, down_a, up_b, down_b]
    for peer in peers:
        pl.semaphore_signal(barrier, inc=1, device_id=peer, device_id_type=MESH)
    far_copy.start()
    near_copy.start()
    dec_ref[mine] = d_ref[...]
    bound_ref[0] = 8.0 * 1.02 * jnp.max(jnp.abs(qg_ref[...] * kg_ref[...]))
    gain = column(qg_ref[...])
    key_gain = column(kg_ref[...])

    first_copies[0].wait()
    rows = x_ref[...].astype(f32)
    scale = lax.rsqrt(jnp.mean(rows * rows, axis=1, keepdims=True) + EPS)
    norm_ref[...] = (rows * scale * in_gain_ref[...]).astype(bf)
    first_copies[1].wait()
    keys = jnp.dot(norm_ref[...], wk_ref[...], preferred_element_type=f32)
    first_copies[2].wait()
    values = jnp.dot(norm_ref[...], wv_ref[...], preferred_element_type=f32)
    keys = head_norm(keys.T, 2, key_gain).astype(bf)
    values = values.T.astype(bf)
    for i in range(2):
        kv_ref[i, 0:64] = keys[i * 64 : (i + 1) * 64]
        kv_ref[i, 64:128] = values[i * 64 : (i + 1) * 64]

    @pl.when(g == c)
    def _():
        all_ref[own_line, tp, 0:128] = kv_ref[g]

    pl.semaphore_wait(barrier, len(peers))

    def decay_copy(k):
        t = lax.rem(mine + k, 4)
        peer = (z, y, 2 * g + t // 2, lax.rem(t, 2))
        return remote(d_ref, dec_ref.at[mine], d_send.at[k], d_recv.at[k], peer)

    def piece_copy(k):
        to = lax.rem(x + k, 4)
        slot = (x - 2 * g) * 2 + c
        return remote(
            kv_ref.at[to // 2],
            all_ref.at[own_line, tp, pl.ds(0, 128)],
            p_send.at[k],
            p_recv.at[slot],
            (z, y, to, g),
        )

    for k in range(1, 4):
        decay_copy(k).start()
    for k in range(1, 4):
        piece_copy(k).start()

    @pl.when(g != c)
    def _():
        piece_copy(0).start()

    def queries(slot):
        flat = jnp.dot(norm_ref[...], wq_ref[slot], preferred_element_type=f32)
        return (head_norm(flat.T, 8, gain) * (LOG2E / 8)).astype(bf)

    far_copy.wait()
    qs_ref[...] = queries(0)

    for k in range(1, 4):
        decay_copy(k).wait_recv()
    for i in range(4):
        first = pl.multiple_of((4 * c + i) * 128, 128)
        value = jnp.concatenate([dec_ref[q, :, pl.ds(first, 128)] for q in range(4)], axis=0)
        all_ref[own_line, 4 * c + i, 128:152] = jnp.concatenate(
            split3(value * LOG2E), axis=0
        ).astype(bf)
    far_first = pl.multiple_of((7 - tp) * 128, 128)
    far_decays = remote(
        dec_ref.at[:, :, pl.ds(far_first, 128)], far_ref, x_send.at[0], x_recv.at[0], across
    )
    far_decays.start()
    q_copy = remote(qs_ref, qr_ref, x_send.at[1], x_recv.at[1], mirror)
    late = own_line < 8

    @pl.when(jnp.logical_not(late))
    def _():
        q_copy.start()

    def block(line, sub):
        return all_ref.at[line, pl.ds(4 * c + 2 * sub, 2)]

    def ring(step, slot):
        side = (0, 0, 0, 0, 3, 1)[slot]
        sub = (0, 1, 0, 1, 0, 1)[slot]
        upward = slot in (0, 1, 4)
        if step == 0:
            line, peer = line_at(side, 0), (up_a if upward else down_a)
        else:
            line, peer = line_at(step - 1, side), (up_b if upward else down_b)
        index = step * 6 + slot
        ref = block(line, sub)
        return remote(ref, ref, r_send.at[index], r_recv.at[index], peer)

    def share(j, k):
        half = all_ref.at[line_at(j, k), pl.ds(4 * c, 4)]
        index = j * 4 + k
        return remote(half, half, s_send.at[index], s_recv.at[index], sibling)

    def ring_start(step):
        for slot in range(4):
            ring(step, slot).start()

    def ring_relay(step):
        ring(step, 0).wait_recv()
        ring(step, 4).start()
        ring(step, 3).wait_recv()
        ring(step, 5).start()
        ring(step, 1).wait_recv()
        ring(step, 2).wait_recv()

    def ring_end(step):
        ring(step, 4).wait_recv()
        ring(step, 5).wait_recv()

    for i in range(4):

        @pl.when(4 * c + i != tp)
        def _():
            remote(
                kv_ref.at[0],
                all_ref.at[own_line, 4 * c + i, pl.ds(0, 128)],
                p_send.at[0],
                p_recv.at[i],
                sibling,
            ).wait_recv()

    ring_start(0)
    ring_start(1)
    share(0, 0).start()

    row8 = lax.broadcasted_iota(jnp.int32, (8, 128), 0)
    ones = jnp.where(row8 < 3, 1.0, 0.0).astype(f32)

    def prepare(rg, query_ref, decays):
        ref_d = jnp.broadcast_to(decays[:, 0:1], (8, 128))
        refd_ref[rg] = ref_d
        parts = split3(decays - ref_d)
        for h in range(8):
            onehot = jnp.where(row8 == h, -1.0, 0.0).astype(f32)
            own = jnp.zeros((8, 128), f32)
            for i, part in enumerate(parts):
                own = jnp.where(row8 == i, part[h : h + 1], own)
            rows = jnp.concatenate([onehot, onehot, onehot, own], axis=0).astype(bf)
            qa_ref[rg, :, h * 128 : (h + 1) * 128] = jnp.concatenate(
                [query_ref[h * 64 : (h + 1) * 64, :], rows, jnp.zeros((32, 128), bf)], axis=0
            )

    near_copy.wait()
    out_copy.start()
    near_ref[...] = queries(1)
    here = pl.multiple_of(tp * 128, 128)
    own_decays = jnp.concatenate([dec_ref[q, :, pl.ds(here, 128)] for q in range(4)], axis=0)
    prepare(0, near_ref, own_decays * LOG2E)
    acc_ref[...] = jnp.zeros_like(acc_ref)
    sum_ref[...] = jnp.zeros_like(sum_ref)
    if not bounded:
        max_ref[...] = jnp.full(max_ref.shape, -1e30, f32)

    def attend(parts, tp_row, masked):
        for i, (rg, line) in enumerate(parts):
            ref_d = refd_ref[rg]
            for p in range(8):
                first = i * 1024 + p * 128
                ka_ref[first : first + 128] = load_keys(all_ref, line, p, ref_d, ones)
        units = [
            (i, m, n)
            for i in range(len(parts))
            for m in range(1024 // ROWS)
            for n in range(1024 // tile)
        ]

        def weigh(u):
            i, m, n = units[u]
            rg = parts[i][0]
            cols = slice(n * tile, (n + 1) * tile)
            first = i * 1024 + m * ROWS
            keys = ka_ref[first : first + ROWS]
            scores = jnp.dot(keys, qa_ref[rg, :, cols], preferred_element_type=f32)
            if masked:
                shape = (ROWS, tile)
                key_pos = m * ROWS + lax.broadcasted_iota(jnp.int32, shape, 0)
                query_pos = tp_row * 128 + (lax.broadcasted_iota(jnp.int32, shape, 1) & 127)
                scores = jnp.where(key_pos <= query_pos, scores, -1e30)
            if bounded:
                weights = jnp.exp2(scores)
                sum_ref[rg, :, cols] += jnp.sum(weights.reshape(ROWS // 8, 8, tile), axis=0)
            else:
                old = max_ref[rg, 0:1, cols]
                new = jnp.maximum(old, jnp.max(scores, axis=0, keepdims=True))
                keep = jnp.exp2(old - new)
                weights = jnp.exp2(scores - new)
                max_ref[rg, :, cols] = jnp.broadcast_to(new, (8, tile))
                sums = jnp.sum(weights.reshape(ROWS // 8, 8, tile), axis=0)
                sum_ref[rg, :, cols] = sum_ref[rg, :, cols] * keep + sums
                acc_ref[rg, :, cols] = acc_ref[rg, :, cols] * keep
            wt_ref[u % (lag + 1)] = weights.astype(bf)

        def gather_values(u):
            i, m, n = units[u]
            rg, line = parts[i]
            cols = slice(n * tile, (n + 1) * tile)
            first = m * ROWS // 128
            values = jnp.concatenate(
                [all_ref[line, p, 64:128] for p in range(first, first + ROWS // 128)], axis=1
            )
            acc_ref[rg, :, cols] += jnp.dot(
                values, wt_ref[u % (lag + 1)], preferred_element_type=f32
            )

        lag = LAG if bounded else 0
        for u in range(len(units) + lag):
            if u < len(units):
                weigh(u)
            if u >= lag:
                gather_values(u - lag)

    def got(step, slot):
        ring(step, slot).wait_recv()

    def pass_on(step, sub):
        for slot in (sub, 2 + sub):
            ring(step, slot).start()

    def act_1():
        got(0, 0)
        ring(0, 4).start()
        pass_on(4, 0)
        got(0, 2)
        pass_on(2, 0)
        got(1, 0)
        ring(1, 4).start()
        got(0, 3)
        ring(0, 5).start()
        pass_on(2, 1)
        got(0, 1)
        pass_on(4, 1)
        share(3, 0).start()
        share(1, 0).start()
        got(1, 3)
        ring(1, 5).start()
        got(1, 1)
        got(1, 2)
        share(0, 3).start()
        share(0, 1).start()

    def act_3():
        got(0, 4)
        pass_on(3, 0)
        got(0, 5)
        pass_on(3, 1)
        share(2, 0).start()
        ring_end(1)
        share(0, 2).start()

    def act_6():
        got(4, 0)
        ring(4, 4).start()
        got(2, 0)
        ring(2, 4).start()
        got(2, 3)
        ring(2, 5).start()
        got(2, 1)
        got(2, 2)
        share(1, 3).start()
        share(1, 1).start()
        got(4, 3)
        ring(4, 5).start()
        got(4, 1)
        got(4, 2)
        share(3, 3).start()
        share(3, 1).start()

        @pl.when(late)
        def _():
            q_copy.start()

    def act_9():
        ring_relay(3)
        share(2, 3).start()
        share(2, 1).start()
        for j in (3, 1):
            ring_end(1 + j)
            share(j, 2).start()

    def act_13():
        ring_end(3)
        share(2, 2).start()

    later = jnp.where(late, 0, 1)
    one = lambda test: test.astype(jnp.int32)

    def wait_half(j, k):
        half = all_ref.at[line_at(j, k), pl.ds(4 * (1 - c), 4)]
        index = k * 4 + j
        remote(half, half, s_send.at[index], s_recv.at[index], sibling).wait_recv()

    far_line = 15 - own_line
    last_line = line_at(2, 2)
    early = jnp.logical_not(late) & (last_line > far_line)

    def back(part):
        rows = pl.ds(part * 256, 256)
        return remote(
            os_ref.at[rows], got_ref.at[rows], x_send.at[2 + part], x_recv.at[2 + part], mirror
        )

    def finish(rg, to_ref):
        inverse = 1.0 / jnp.sum(sum_ref[rg], axis=0, keepdims=True)
        for h in range(8):
            cols = slice(h * 128, (h + 1) * 128)
            to_ref[h * 64 : (h + 1) * 64, :] = (acc_ref[rg, :, cols] * inverse[:, cols]).astype(bf)

    wait_half(0, 0)
    attend([(0, own_line)], tp, True)

    def body(group, carry):
        actions = ((0, act_1), (1 + later, act_3), (2 + later, act_6), (4, act_9), (6 + later, act_13))
        for at, action in actions:

            @pl.when(group == at)
            def _(action=action):
                action()

        @pl.when((group == 6) & early)
        def _():
            for part in range(2):
                back(part).start()

        for at, members in enumerate(GROUPS):

            @pl.when(group == (at + later if at == 6 else at))
            def _(members=members):
                for j, k in members:
                    if (j, k) != (0, 0):
                        wait_half(j, k)

        @pl.when(group == 5 * later)
        def _():
            far_decays.wait_recv()
            q_copy.wait_recv()
            far = jnp.concatenate([far_ref[q] for q in range(4)], axis=0)
            prepare(1, qr_ref, far * LOG2E)

        turn = group + later * (2 * one(group == 5) - one(group > 5))
        again = one(turn == 7)
        size = unpacked((3, 2, 2, 2, 2, 4, 1, 0), turn)
        lines = []
        for i in range(4):
            pick = lambda axis: unpacked(
                [g[i][axis] if i < len(g) else 0 for g in GROUPS] + [0], turn
            )
            lines.append(line_at(pick(0), pick(1)))
        flags = []
        for i in range(4):
            here = one(i < size)
            flags.append(here * one(lines[i] < own_line))
            flags.append(here * one(lines[i] < far_line) * jnp.where(turn == 6, 1, 1 - later))
        before, count = [], 0
        for flag in flags:
            before.append(count)
            count = count + flag
        count = count * (1 - again) + (far_line - one(last_line < far_line)) * again

        def unit(index):
            rg, line = again, (index + one(index >= last_line)) * again
            for i in range(8):
                chosen = flags[i] * one(before[i] == index)
                line = line + chosen * lines[i // 2]
                if i % 2:
                    rg = rg + chosen
            return rg, line

        def pair(index, inner):
            attend([unit(2 * index), unit(2 * index + 1)], tp, False)
            return inner

        lax.fori_loop(0, count // 2, pair, 0)

        @pl.when((count & 1) == 1)
        def _():
            attend([unit(count - 1)], tp, False)

        @pl.when(group == 4 + later)
        def _():
            attend([(1, far_line)], 7 - tp, True)

        @pl.when((group == 5) & early)
        def _():
            finish(1, os_ref)

        return carry

    lax.fori_loop(0, 7 + later, body, 0)

    @pl.when(jnp.logical_not(early))
    def _():
        finish(1, os_ref)

    finish(0, near_ref)

    @pl.when(jnp.logical_not(early))
    def _():
        for part in range(2):
            back(part).start()

    out_copy.wait()
    near = near_ref[...].T
    for n in range(4):
        cols = slice(n * 512, (n + 1) * 512)
        part_ref[:, cols] = jnp.dot(near, wo_ref[pl.ds(w_near, 512), cols], preferred_element_type=f32)
    for k in range(1, 4):
        decay_copy(k).wait_send()
        piece_copy(k).wait_send()

    @pl.when(g != c)
    def _():
        piece_copy(0).wait_send()

    far_decays.wait_send()
    q_copy.wait_send()
    for step in range(5):
        for slot in range(6):
            ring(step, slot).wait_send()
    for j in range(4):
        for k in range(4):
            share(j, k).wait_send()
    for part in range(2):
        back(part).wait_recv()
        far = got_ref[part * 256 : (part + 1) * 256, :].T
        rows = pl.ds(pl.multiple_of(w_far + part * 256, 256), 256)
        for n in range(2):
            cols = slice(n * 1024, (n + 1) * 1024)
            rest = jnp.dot(far, wo_ref[rows, cols], preferred_element_type=f32)
            if part == 0:
                part_ref[:, cols] += rest
            else:
                out_ref[:, cols] = (part_ref[:, cols] + rest).astype(bf)
    for part in range(2):
        back(part).wait_send()


def main(x, in_gain, wk, wv, qg, kg, d, wq, wo, bounded):
    dma = lambda *n: pltpu.SemaphoreType.DMA(n)
    return pl.pallas_call(
        functools.partial(main_kernel, bounded, 512),
        out_shape=[jax.ShapeDtypeStruct((128, 2048), bf), jax.ShapeDtypeStruct((1,), f32)],
        in_specs=[HBM, VM, HBM, HBM, VM, VM, VM, HBM, HBM],
        out_specs=[VM, pl.BlockSpec(memory_space=pltpu.SMEM)],
        scratch_shapes=[
            pltpu.VMEM((128, 2048), bf),
            pltpu.VMEM((2048, 128), bf),
            pltpu.VMEM((2048, 128), bf),
            pltpu.VMEM((128, 2048), bf),
            pltpu.VMEM((2, 128, 128), bf),
            pltpu.VMEM((16, 8, 152, 128), bf),
            pltpu.VMEM((4, 2, 1024), f32),
            pltpu.VMEM((4, 2, 128), f32),
            pltpu.VMEM((2, 2048, 512), bf),
            pltpu.VMEM((1024, 2048), bf),
            pltpu.VMEM((128, 2048), f32),
            pltpu.VMEM((512, 128), bf),
            pltpu.VMEM((512, 128), bf),
            pltpu.VMEM((512, 128), bf),
            pltpu.VMEM((512, 128), bf),
            pltpu.VMEM((512, 128), bf),
            pltpu.VMEM((2, 128, 1024), bf),
            pltpu.VMEM((2, 64, 1024), f32),
            pltpu.VMEM((2, 8, 1024), f32),
            pltpu.VMEM((2, 8, 1024), f32),
            pltpu.VMEM((2, 8, 128), f32),
            pltpu.VMEM((2048, 128), bf),
            pltpu.VMEM((LAG + 1, ROWS, 512), bf),
            dma(6),
            dma(4),
            dma(4),
            dma(4),
            dma(4),
            dma(4),
            dma(4),
            dma(30),
            dma(30),
            dma(16),
            dma(16),
        ],
        compiler_params=pltpu.CompilerParams(
            collective_id=0 if bounded else 1,
            has_side_effects=True,
            vmem_limit_bytes=67_000_000,
        ),
        name="main_bounded" if bounded else "main_any",
    )(x, in_gain, wk, wv, qg, kg, d, wq, wo)


def per_device(inputs, in_gain, w_query, w_key, w_value, query_gain, key_gain, decay_sums, w_out):
    args = (
        inputs,
        in_gain.reshape(1, -1),
        w_key,
        w_value,
        query_gain.reshape(1, -1),
        key_gain.reshape(1, -1),
        decay_sums.T,
        w_query,
        w_out,
    )
    result, bound = main(*args, True)
    return lax.cond(
        bound[0] <= 64.0, lambda kept, *a: kept, lambda kept, *a: main(*a, False)[0], result, *args
    )


def solution(mesh):
    torus = Mesh(mesh.devices.reshape(4, 4, 4, 2), ("z", "y", "x", "c"))
    every = ("z", "y", "x", "c")
    in_specs = (P(every, None), P(), P(), P(), P(), P(), P(), P(("z", "y"), ("x", "c")), P())
    return jax.shard_map(
        per_device, mesh=torus, in_specs=in_specs, out_specs=P(every, None), check_vma=False
    )
```

```python
import functools

import jax
import jax.numpy as jnp
from jax import lax
from jax.experimental import pallas as pl
from jax.experimental.pallas import tpu as pltpu
from jax.sharding import Mesh
from jax.sharding import PartitionSpec as P

f32 = jnp.float32
bf = jnp.bfloat16
LOG2E = 1.4426950408889634
EPS = 1e-06
MESH = pl.DeviceIdType.MESH
VM = pl.BlockSpec(memory_space=pltpu.VMEM)


def split3(x):
    high = x.astype(bf).astype(f32)
    rest = x - high
    mid = rest.astype(bf).astype(f32)
    return high, mid, rest - mid


def head_norm(flat, heads, gain):
    x = flat.reshape(heads, 64, flat.shape[1])
    scale = lax.rsqrt(jnp.mean(x * x, axis=1, keepdims=True) + EPS)
    return (x * scale * gain[None]).reshape(flat.shape)


HBM = pl.BlockSpec(memory_space=pltpu.HBM)
GROUPS = (
    ((0, 0), (3, 0), (0, 3)),
    ((1, 0), (0, 1)),
    ((2, 0), (0, 2)),
    ((3, 3), (1, 3)),
    ((3, 1), (1, 1)),
    ((3, 2), (1, 2), (2, 3), (2, 1)),
    ((2, 2),),
)
ROWS, LAG = 256, 3


def packed(values):
    total = sum(v << 4 * i for i, v in enumerate(values))
    return total - (1 << 32) if total >> 31 else total


def unpacked(values, index):
    return lax.shift_right_logical(jnp.int32(packed(values)), 4 * index) & 15


def column(row):
    return jnp.broadcast_to(row, (128, 64)).T


def load_keys(all_ref, line, p, ref_d, ones):
    dec = all_ref[line, p, 128:152].astype(f32)
    rel = dec[0:8] + dec[8:16] + dec[16:24] - ref_d
    rows = jnp.concatenate([*split3(rel), ones], axis=0).astype(bf)
    full = jnp.concatenate([all_ref[line, p, 0:64], rows, jnp.zeros((32, 128), bf)], axis=0)
    return full.T


def main_kernel(bounded, tile, *refs):
    x_hbm, in_gain_ref, wk_hbm, wv_hbm, qg_ref, kg_ref, d_ref, wq_hbm, wo_hbm = refs[:9]
    out_ref, bound_ref = refs[9:11]
    x_ref, wk_ref, wv_ref, norm_ref, kv_ref = refs[11:16]
    scratch = refs[16:]
    all_ref, dec_ref, far_ref, wq_ref, wo_ref, part_ref = scratch[:6]
    qs_ref, qr_ref, os_ref, near_ref, got_ref = scratch[6:11]
    qa_ref, acc_ref, sum_ref, max_ref, refd_ref, ka_ref, wt_ref = scratch[11:18]
    w_sem, p_send, p_recv, d_send, d_recv, x_send, x_recv, r_send, r_recv, s_send, s_recv = scratch[18:]
    z, y, x, c = (lax.axis_index(n) for n in ("z", "y", "x", "c"))
    g = x // 2
    tp = 2 * x + c
    own_line = 4 * z + y
    mine = (x - 2 * g) * 2 + c
    mirror = (3 - z, 3 - y, 3 - x, 1 - c)
    across = (3 - z, 3 - y, x, c)
    sibling = (z, y, x, 1 - c)
    a = (1 - c) * y + c * z
    b = (1 - c) * z + c * y

    def line_at(j, k):
        pa, pb = (a + j) & 3, (b + k) & 3
        return (1 - c) * (4 * pb + pa) + c * (4 * pa + pb)

    def at_ab(j, k):
        pa, pb = (a + j) & 3, (b + k) & 3
        return ((1 - c) * pb + c * pa, (1 - c) * pa + c * pb, x, c)

    up_a, down_a, up_b, down_b = at_ab(1, 0), at_ab(3, 0), at_ab(0, 1), at_ab(0, 3)

    def remote(src, dst, send_sem, recv_sem, peer):
        return pltpu.make_async_remote_copy(
            src_ref=src,
            dst_ref=dst,
            send_sem=send_sem,
            recv_sem=recv_sem,
            device_id=peer,
            device_id_type=MESH,
        )

    w_far = pl.multiple_of((1 - g) * 512, 512)
    w_near = pl.multiple_of(g * 512, 512)
    far_copy = pltpu.make_async_copy(wq_hbm.at[:, pl.ds(w_far, 512)], wq_ref.at[0], w_sem.at[0])
    near_copy = pltpu.make_async_copy(wq_hbm.at[:, pl.ds(w_near, 512)], wq_ref.at[1], w_sem.at[1])
    out_copy = pltpu.make_async_copy(wo_hbm, wo_ref, w_sem.at[2])

    first_copies = [
        pltpu.make_async_copy(src, dst, w_sem.at[3 + i])
        for i, (src, dst) in enumerate(((x_hbm, x_ref), (wk_hbm, wk_ref), (wv_hbm, wv_ref)))
    ]
    for copy in first_copies:
        copy.start()
    barrier = pltpu.get_barrier_semaphore()
    peers = [(z, y, lax.rem(x + k, 4), cc) for k in range(1, 4) for cc in range(2)]
    peers += [sibling, mirror, across, up_a, down_a, up_b, down_b]
    for peer in peers:
        pl.semaphore_signal(barrier, inc=1, device_id=peer, device_id_type=MESH)
    far_copy.start()
    near_copy.start()
    dec_ref[mine] = d_ref[...]
    bound_ref[0] = 8.0 * 1.02 * jnp.max(jnp.abs(qg_ref[...] * kg_ref[...]))
    gain = column(qg_ref[...])
    key_gain = column(kg_ref[...])

    first_copies[0].wait()
    rows = x_ref[...].astype(f32)
    scale = lax.rsqrt(jnp.mean(rows * rows, axis=1, keepdims=True) + EPS)
    norm_ref[...] = (rows * scale * in_gain_ref[...]).astype(bf)
    first_copies[1].wait()
    keys = jnp.dot(norm_ref[...], wk_ref[...], preferred_element_type=f32)
    first_copies[2].wait()
    values = jnp.dot(norm_ref[...], wv_ref[...], preferred_element_type=f32)
    keys = head_norm(keys.T, 2, key_gain).astype(bf)
    values = values.T.astype(bf)
    for i in range(2):
        kv_ref[i, 0:64] = keys[i * 64 : (i + 1) * 64]
        kv_ref[i, 64:128] = values[i * 64 : (i + 1) * 64]

    @pl.when(g == c)
    def _():
        all_ref[own_line, tp, 0:128] = kv_ref[g]

    pl.semaphore_wait(barrier, len(peers))

    def decay_copy(k):
        t = lax.rem(mine + k, 4)
        peer = (z, y, 2 * g + t // 2, lax.rem(t, 2))
        return remote(d_ref, dec_ref.at[mine], d_send.at[k], d_recv.at[k], peer)

    def piece_copy(k):
        to = lax.rem(x + k, 4)
        slot = (x - 2 * g) * 2 + c
        return remote(
            kv_ref.at[to // 2],
            all_ref.at[own_line, tp, pl.ds(0, 128)],
            p_send.at[k],
            p_recv.at[slot],
            (z, y, to, g),
        )

    for k in range(1, 4):
        decay_copy(k).start()
    for k in range(1, 4):
        piece_copy(k).start()

    @pl.when(g != c)
    def _():
        piece_copy(0).start()

    def queries(slot):
        flat = jnp.dot(norm_ref[...], wq_ref[slot], preferred_element_type=f32)
        return (head_norm(flat.T, 8, gain) * (LOG2E / 8)).astype(bf)

    far_copy.wait()
    qs_ref[...] = queries(0)

    for k in range(1, 4):
        decay_copy(k).wait_recv()
    for i in range(4):
        first = pl.multiple_of((4 * c + i) * 128, 128)
        value = jnp.concatenate([dec_ref[q, :, pl.ds(first, 128)] for q in range(4)], axis=0)
        all_ref[own_line, 4 * c + i, 128:152] = jnp.concatenate(
            split3(value * LOG2E), axis=0
        ).astype(bf)
    far_first = pl.multiple_of((7 - tp) * 128, 128)
    far_decays = remote(
        dec_ref.at[:, :, pl.ds(far_first, 128)], far_ref, x_send.at[0], x_recv.at[0], across
    )
    far_decays.start()
    q_copy = remote(qs_ref, qr_ref, x_send.at[1], x_recv.at[1], mirror)
    late = own_line < 8

    @pl.when(jnp.logical_not(late))
    def _():
        q_copy.start()

    def block(line, sub):
        return all_ref.at[line, pl.ds(4 * c + 2 * sub, 2)]

    def ring(step, slot):
        side = (0, 0, 0, 0, 3, 1)[slot]
        sub = (0, 1, 0, 1, 0, 1)[slot]
        upward = slot in (0, 1, 4)
        if step == 0:
            line, peer = line_at(side, 0), (up_a if upward else down_a)
        else:
            line, peer = line_at(step - 1, side), (up_b if upward else down_b)
        index = step * 6 + slot
        ref = block(line, sub)
        return remote(ref, ref, r_send.at[index], r_recv.at[index], peer)

    def share(j, k):
        half = all_ref.at[line_at(j, k), pl.ds(4 * c, 4)]
        index = j * 4 + k
        return remote(half, half, s_send.at[index], s_recv.at[index], sibling)

    def ring_start(step):
        for slot in range(4):
            ring(step, slot).start()

    def ring_relay(step):
        ring(step, 0).wait_recv()
        ring(step, 4).start()
        ring(step, 3).wait_recv()
        ring(step, 5).start()
        ring(step, 1).wait_recv()
        ring(step, 2).wait_recv()

    def ring_end(step):
        ring(step, 4).wait_recv()
        ring(step, 5).wait_recv()

    for i in range(4):

        @pl.when(4 * c + i != tp)
        def _():
            remote(
                kv_ref.at[0],
                all_ref.at[own_line, 4 * c + i, pl.ds(0, 128)],
                p_send.at[0],
                p_recv.at[i],
                sibling,
            ).wait_recv()

    ring_start(0)
    ring_start(1)
    share(0, 0).start()

    row8 = lax.broadcasted_iota(jnp.int32, (8, 128), 0)
    ones = jnp.where(row8 < 3, 1.0, 0.0).astype(f32)

    def prepare(rg, query_ref, decays):
        ref_d = jnp.broadcast_to(decays[:, 0:1], (8, 128))
        refd_ref[rg] = ref_d
        parts = split3(decays - ref_d)
        for h in range(8):
            onehot = jnp.where(row8 == h, -1.0, 0.0).astype(f32)
            own = jnp.zeros((8, 128), f32)
            for i, part in enumerate(parts):
                own = jnp.where(row8 == i, part[h : h + 1], own)
            rows = jnp.concatenate([onehot, onehot, onehot, own], axis=0).astype(bf)
            qa_ref[rg, :, h * 128 : (h + 1) * 128] = jnp.concatenate(
                [query_ref[h * 64 : (h + 1) * 64, :], rows, jnp.zeros((32, 128), bf)], axis=0
            )

    near_copy.wait()
    out_copy.start()
    near_ref[...] = queries(1)
    here = pl.multiple_of(tp * 128, 128)
    own_decays = jnp.concatenate([dec_ref[q, :, pl.ds(here, 128)] for q in range(4)], axis=0)
    prepare(0, near_ref, own_decays * LOG2E)
    acc_ref[...] = jnp.zeros_like(acc_ref)
    sum_ref[...] = jnp.zeros_like(sum_ref)
    if not bounded:
        max_ref[...] = jnp.full(max_ref.shape, -1e30, f32)

    def attend(parts, tp_row, masked):
        for i, (rg, line) in enumerate(parts):
            ref_d = refd_ref[rg]
            for p in range(8):
                first = i * 1024 + p * 128
                ka_ref[first : first + 128] = load_keys(all_ref, line, p, ref_d, ones)
        units = [
            (i, m, n)
            for i in range(len(parts))
            for m in range(1024 // ROWS)
            for n in range(1024 // tile)
        ]

        def weigh(u):
            i, m, n = units[u]
            rg = parts[i][0]
            cols = slice(n * tile, (n + 1) * tile)
            first = i * 1024 + m * ROWS
            keys = ka_ref[first : first + ROWS]
            scores = jnp.dot(keys, qa_ref[rg, :, cols], preferred_element_type=f32)
            if masked:
                shape = (ROWS, tile)
                key_pos = m * ROWS + lax.broadcasted_iota(jnp.int32, shape, 0)
                query_pos = tp_row * 128 + (lax.broadcasted_iota(jnp.int32, shape, 1) & 127)
                scores = jnp.where(key_pos <= query_pos, scores, -1e30)
            if bounded:
                weights = jnp.exp2(scores)
                sum_ref[rg, :, cols] += jnp.sum(weights.reshape(ROWS // 8, 8, tile), axis=0)
            else:
                old = max_ref[rg, 0:1, cols]
                new = jnp.maximum(old, jnp.max(scores, axis=0, keepdims=True))
                keep = jnp.exp2(old - new)
                weights = jnp.exp2(scores - new)
                max_ref[rg, :, cols] = jnp.broadcast_to(new, (8, tile))
                sums = jnp.sum(weights.reshape(ROWS // 8, 8, tile), axis=0)
                sum_ref[rg, :, cols] = sum_ref[rg, :, cols] * keep + sums
                acc_ref[rg, :, cols] = acc_ref[rg, :, cols] * keep
            wt_ref[u % (lag + 1)] = weights.astype(bf)

        def gather_values(u):
            i, m, n = units[u]
            rg, line = parts[i]
            cols = slice(n * tile, (n + 1) * tile)
            first = m * ROWS // 128
            values = jnp.concatenate(
                [all_ref[line, p, 64:128] for p in range(first, first + ROWS // 128)], axis=1
            )
            acc_ref[rg, :, cols] += jnp.dot(
                values, wt_ref[u % (lag + 1)], preferred_element_type=f32
            )

        lag = LAG if bounded else 0
        for u in range(len(units) + lag):
            if u < len(units):
                weigh(u)
            if u >= lag:
                gather_values(u - lag)

    def got(step, slot):
        ring(step, slot).wait_recv()

    def pass_on(step, sub):
        for slot in (sub, 2 + sub):
            ring(step, slot).start()

    def act_1():
        got(0, 0)
        ring(0, 4).start()
        pass_on(4, 0)
        got(0, 2)
        pass_on(2, 0)
        got(1, 0)
        ring(1, 4).start()
        got(0, 3)
        ring(0, 5).start()
        pass_on(2, 1)
        got(0, 1)
        pass_on(4, 1)
        share(3, 0).start()
        share(1, 0).start()
        got(1, 3)
        ring(1, 5).start()
        got(1, 1)
        got(1, 2)
        share(0, 3).start()
        share(0, 1).start()

    def act_3():
        got(0, 4)
        pass_on(3, 0)
        got(0, 5)
        pass_on(3, 1)
        share(2, 0).start()
        ring_end(1)
        share(0, 2).start()

    def act_6():
        got(4, 0)
        ring(4, 4).start()
        got(2, 0)
        ring(2, 4).start()
        got(2, 3)
        ring(2, 5).start()
        got(2, 1)
        got(2, 2)
        share(1, 3).start()
        share(1, 1).start()
        got(4, 3)
        ring(4, 5).start()
        got(4, 1)
        got(4, 2)
        share(3, 3).start()
        share(3, 1).start()

        @pl.when(late)
        def _():
            q_copy.start()

    def act_9():
        ring_relay(3)
        share(2, 3).start()
        share(2, 1).start()
        for j in (3, 1):
            ring_end(1 + j)
            share(j, 2).start()

    def act_13():
        ring_end(3)
        share(2, 2).start()

    later = jnp.where(late, 0, 1)
    one = lambda test: test.astype(jnp.int32)

    def wait_half(j, k):
        half = all_ref.at[line_at(j, k), pl.ds(4 * (1 - c), 4)]
        index = k * 4 + j
        remote(half, half, s_send.at[index], s_recv.at[index], sibling).wait_recv()

    far_line = 15 - own_line
    last_line = line_at(2, 2)
    early = jnp.logical_not(late) & (last_line > far_line)
    hold = jnp.logical_not(late) & (last_line <= far_line)

    def back(part):
        rows = pl.ds(part * 256, 256)
        return remote(
            os_ref.at[rows], got_ref.at[rows], x_send.at[2 + part], x_recv.at[2 + part], mirror
        )

    def finish(rg, to_ref):
        inverse = 1.0 / jnp.sum(sum_ref[rg], axis=0, keepdims=True)
        for h in range(8):
            cols = slice(h * 128, (h + 1) * 128)
            to_ref[h * 64 : (h + 1) * 64, :] = (acc_ref[rg, :, cols] * inverse[:, cols]).astype(bf)

    wait_half(0, 0)
    attend([(0, own_line)], tp, True)

    def body(group, carry):
        actions = ((0, act_1), (1 + later, act_3), (2 + later, act_6), (4, act_9), (6 + one(early), act_13))
        for at, action in actions:

            @pl.when(group == at)
            def _(action=action):
                action()

        @pl.when(group == jnp.where(late, 99, 6 + one(hold)))
        def _():
            for part in range(2):
                back(part).start()

        for at, members in enumerate(GROUPS):

            @pl.when(group == (at + one(early) if at == 6 else at))
            def _(members=members):
                for j, k in members:
                    if (j, k) != (0, 0):
                        wait_half(j, k)

        @pl.when(group == 5 * later)
        def _():
            far_decays.wait_recv()
            q_copy.wait_recv()
            far = jnp.concatenate([far_ref[q] for q in range(4)], axis=0)
            prepare(1, qr_ref, far * LOG2E)

        turn = group + later * (2 * one(group == 5) - one(group > 5) * one(early))
        turn = turn - 2 * one(hold) * one(group == 7)
        again = one(turn == 7)
        size = unpacked((3, 2, 2, 2, 2, 4, 1, 0), turn)
        lines = []
        for i in range(4):
            pick = lambda axis: unpacked(
                [g[i][axis] if i < len(g) else 0 for g in GROUPS] + [0], turn
            )
            lines.append(line_at(pick(0), pick(1)))
        flags = []
        for i in range(4):
            here = one(i < size)
            flags.append(here * one(lines[i] < own_line) * (1 - one(hold) * one(group == 6)))
            flags.append(here * one(lines[i] < far_line) * jnp.where(turn == 6, 1, 1 - later))
        lines.append(last_line)
        flags.append(one(last_line < own_line) * one(hold) * one(group == 7))
        before, count = [], 0
        for flag in flags:
            before.append(count)
            count = count + flag
        count = count * (1 - again) + (far_line - one(last_line < far_line)) * again

        def unit(index):
            rg, line = again, (index + one(index >= last_line)) * again
            for i in range(9):
                chosen = flags[i] * one(before[i] == index)
                line = line + chosen * lines[i // 2]
                if i % 2:
                    rg = rg + chosen
            return rg, line

        def pair(index, inner):
            attend([unit(2 * index), unit(2 * index + 1)], tp, False)
            return inner

        lax.fori_loop(0, count // 2, pair, 0)

        @pl.when((count & 1) == 1)
        def _():
            attend([unit(count - 1)], tp, False)

        @pl.when(group == 4 + later)
        def _():
            attend([(1, far_line)], 7 - tp, True)

        @pl.when(group == jnp.where(late, 99, 5 + one(hold)))
        def _():
            finish(1, os_ref)

        return carry

    lax.fori_loop(0, 7 + later, body, 0)

    @pl.when(late)
    def _():
        finish(1, os_ref)

    finish(0, near_ref)

    @pl.when(late)
    def _():
        for part in range(2):
            back(part).start()

    out_copy.wait()
    near = near_ref[...].T
    for n in range(4):
        cols = slice(n * 512, (n + 1) * 512)
        part_ref[:, cols] = jnp.dot(near, wo_ref[pl.ds(w_near, 512), cols], preferred_element_type=f32)
    for k in range(1, 4):
        decay_copy(k).wait_send()
        piece_copy(k).wait_send()

    @pl.when(g != c)
    def _():
        piece_copy(0).wait_send()

    far_decays.wait_send()
    q_copy.wait_send()
    for step in range(5):
        for slot in range(6):
            ring(step, slot).wait_send()
    for j in range(4):
        for k in range(4):
            share(j, k).wait_send()
    for part in range(2):
        back(part).wait_recv()
        far = got_ref[part * 256 : (part + 1) * 256, :].T
        rows = pl.ds(pl.multiple_of(w_far + part * 256, 256), 256)
        for n in range(2):
            cols = slice(n * 1024, (n + 1) * 1024)
            rest = jnp.dot(far, wo_ref[rows, cols], preferred_element_type=f32)
            if part == 0:
                part_ref[:, cols] += rest
            else:
                out_ref[:, cols] = (part_ref[:, cols] + rest).astype(bf)
    for part in range(2):
        back(part).wait_send()


def main(x, in_gain, wk, wv, qg, kg, d, wq, wo, bounded):
    dma = lambda *n: pltpu.SemaphoreType.DMA(n)
    return pl.pallas_call(
        functools.partial(main_kernel, bounded, 512),
        out_shape=[jax.ShapeDtypeStruct((128, 2048), bf), jax.ShapeDtypeStruct((1,), f32)],
        in_specs=[HBM, VM, HBM, HBM, VM, VM, VM, HBM, HBM],
        out_specs=[VM, pl.BlockSpec(memory_space=pltpu.SMEM)],
        scratch_shapes=[
            pltpu.VMEM((128, 2048), bf),
            pltpu.VMEM((2048, 128), bf),
            pltpu.VMEM((2048, 128), bf),
            pltpu.VMEM((128, 2048), bf),
            pltpu.VMEM((2, 128, 128), bf),
            pltpu.VMEM((16, 8, 152, 128), bf),
            pltpu.VMEM((4, 2, 1024), f32),
            pltpu.VMEM((4, 2, 128), f32),
            pltpu.VMEM((2, 2048, 512), bf),
            pltpu.VMEM((1024, 2048), bf),
            pltpu.VMEM((128, 2048), f32),
            pltpu.VMEM((512, 128), bf),
            pltpu.VMEM((512, 128), bf),
            pltpu.VMEM((512, 128), bf),
            pltpu.VMEM((512, 128), bf),
            pltpu.VMEM((512, 128), bf),
            pltpu.VMEM((2, 128, 1024), bf),
            pltpu.VMEM((2, 64, 1024), f32),
            pltpu.VMEM((2, 8, 1024), f32),
            pltpu.VMEM((2, 8, 1024), f32),
            pltpu.VMEM((2, 8, 128), f32),
            pltpu.VMEM((2048, 128), bf),
            pltpu.VMEM((LAG + 1, ROWS, 512), bf),
            dma(6),
            dma(4),
            dma(4),
            dma(4),
            dma(4),
            dma(4),
            dma(4),
            dma(30),
            dma(30),
            dma(16),
            dma(16),
        ],
        compiler_params=pltpu.CompilerParams(
            collective_id=0 if bounded else 1,
            has_side_effects=True,
            vmem_limit_bytes=60 * 1024 * 1024,
        ),
        name="main_bounded" if bounded else "main_any",
    )(x, in_gain, wk, wv, qg, kg, d, wq, wo)


def per_device(inputs, in_gain, w_query, w_key, w_value, query_gain, key_gain, decay_sums, w_out):
    args = (
        inputs,
        in_gain.reshape(1, -1),
        w_key,
        w_value,
        query_gain.reshape(1, -1),
        key_gain.reshape(1, -1),
        decay_sums.T,
        w_query,
        w_out,
    )
    result, bound = main(*args, True)
    return lax.cond(
        bound[0] <= 64.0, lambda kept, *a: kept, lambda kept, *a: main(*a, False)[0], result, *args
    )


def solution(mesh):
    torus = Mesh(mesh.devices.reshape(4, 4, 4, 2), ("z", "y", "x", "c"))
    every = ("z", "y", "x", "c")
    in_specs = (P(every, None), P(), P(), P(), P(), P(), P(), P(("z", "y"), ("x", "c")), P())
    return jax.shard_map(
        per_device, mesh=torus, in_specs=in_specs, out_specs=P(every, None), check_vma=False
    )
```

```python
import functools

import jax
import jax.numpy as jnp
from jax import lax
from jax.experimental import pallas as pl
from jax.experimental.pallas import tpu as pltpu
from jax.sharding import Mesh
from jax.sharding import PartitionSpec as P

f32 = jnp.float32
bf = jnp.bfloat16
LOG2E = 1.4426950408889634
EPS = 1e-06
MESH = pl.DeviceIdType.MESH
VM = pl.BlockSpec(memory_space=pltpu.VMEM)


def split3(x):
    high = x.astype(bf).astype(f32)
    rest = x - high
    mid = rest.astype(bf).astype(f32)
    return high, mid, rest - mid


def head_norm(flat, heads, gain):
    x = flat.reshape(heads, 64, flat.shape[1])
    scale = lax.rsqrt(jnp.mean(x * x, axis=1, keepdims=True) + EPS)
    return (x * scale * gain[None]).reshape(flat.shape)


HBM = pl.BlockSpec(memory_space=pltpu.HBM)
GROUPS = (
    ((0, 0), (3, 0), (0, 3)),
    ((1, 0), (0, 1)),
    ((2, 0), (0, 2)),
    ((3, 3), (1, 3)),
    ((3, 1), (1, 1)),
    ((3, 2), (1, 2), (2, 3), (2, 1)),
    ((2, 2),),
)
ROWS, LAG = 256, 3


def packed(values):
    total = sum(v << 4 * i for i, v in enumerate(values))
    return total - (1 << 32) if total >> 31 else total


def unpacked(values, index):
    return lax.shift_right_logical(jnp.int32(packed(values)), 4 * index) & 15


def column(row):
    return jnp.broadcast_to(row, (128, 64)).T


def load_keys(all_ref, line, p, ref_d, ones):
    dec = all_ref[line, p, 128:152].astype(f32)
    rel = dec[0:8] + dec[8:16] + dec[16:24] - ref_d
    rows = jnp.concatenate([*split3(rel), ones], axis=0).astype(bf)
    full = jnp.concatenate([all_ref[line, p, 0:64], rows, jnp.zeros((32, 128), bf)], axis=0)
    return full.T


def main_kernel(bounded, tile, *refs):
    x_hbm, in_gain_ref, wk_hbm, wv_hbm, qg_ref, kg_ref, d_ref, wq_hbm, wo_hbm = refs[:9]
    out_ref, bound_ref = refs[9:11]
    x_ref, wk_ref, wv_ref, norm_ref, kv_ref = refs[11:16]
    scratch = refs[16:]
    all_ref, dec_ref, far_ref, wq_ref, wo_ref, part_ref = scratch[:6]
    qs_ref, qr_ref, os_ref, near_ref, got_ref = scratch[6:11]
    qa_ref, acc_ref, sum_ref, max_ref, refd_ref, ka_ref, wt_ref = scratch[11:18]
    w_sem, p_send, p_recv, d_send, d_recv, x_send, x_recv, r_send, r_recv, s_send, s_recv = scratch[18:]
    z, y, x, c = (lax.axis_index(n) for n in ("z", "y", "x", "c"))
    g = x // 2
    tp = 2 * x + c
    own_line = 4 * z + y
    mine = (x - 2 * g) * 2 + c
    mirror = (3 - z, 3 - y, 3 - x, 1 - c)
    across = (3 - z, 3 - y, x, c)
    sibling = (z, y, x, 1 - c)
    a = (1 - c) * y + c * z
    b = (1 - c) * z + c * y

    def line_at(j, k):
        pa, pb = (a + j) & 3, (b + k) & 3
        return (1 - c) * (4 * pb + pa) + c * (4 * pa + pb)

    def at_ab(j, k):
        pa, pb = (a + j) & 3, (b + k) & 3
        return ((1 - c) * pb + c * pa, (1 - c) * pa + c * pb, x, c)

    up_a, down_a, up_b, down_b = at_ab(1, 0), at_ab(3, 0), at_ab(0, 1), at_ab(0, 3)

    def remote(src, dst, send_sem, recv_sem, peer):
        return pltpu.make_async_remote_copy(
            src_ref=src,
            dst_ref=dst,
            send_sem=send_sem,
            recv_sem=recv_sem,
            device_id=peer,
            device_id_type=MESH,
        )

    w_far = pl.multiple_of((1 - g) * 512, 512)
    w_near = pl.multiple_of(g * 512, 512)
    far_copy = pltpu.make_async_copy(wq_hbm.at[:, pl.ds(w_far, 512)], wq_ref.at[0], w_sem.at[0])
    near_copy = pltpu.make_async_copy(wq_hbm.at[:, pl.ds(w_near, 512)], wq_ref.at[1], w_sem.at[1])
    out_copy = pltpu.make_async_copy(wo_hbm, wo_ref, w_sem.at[2])

    first_copies = [
        pltpu.make_async_copy(src, dst, w_sem.at[3 + i])
        for i, (src, dst) in enumerate(((x_hbm, x_ref), (wk_hbm, wk_ref), (wv_hbm, wv_ref)))
    ]
    for copy in first_copies:
        copy.start()
    barrier = pltpu.get_barrier_semaphore()
    peers = [(z, y, lax.rem(x + k, 4), cc) for k in range(1, 4) for cc in range(2)]
    peers += [sibling, mirror, across, up_a, down_a, up_b, down_b]
    for peer in peers:
        pl.semaphore_signal(barrier, inc=1, device_id=peer, device_id_type=MESH)
    far_copy.start()
    near_copy.start()
    dec_ref[mine] = d_ref[...]
    bound_ref[0] = 8.0 * 1.02 * jnp.max(jnp.abs(qg_ref[...] * kg_ref[...]))
    gain = column(qg_ref[...])
    key_gain = column(kg_ref[...])

    first_copies[0].wait()
    rows = x_ref[...].astype(f32)
    scale = lax.rsqrt(jnp.mean(rows * rows, axis=1, keepdims=True) + EPS)
    norm_ref[...] = (rows * scale * in_gain_ref[...]).astype(bf)
    first_copies[1].wait()
    keys = jnp.dot(norm_ref[...], wk_ref[...], preferred_element_type=f32)
    first_copies[2].wait()
    values = jnp.dot(norm_ref[...], wv_ref[...], preferred_element_type=f32)
    keys = head_norm(keys.T, 2, key_gain).astype(bf)
    values = values.T.astype(bf)
    for i in range(2):
        kv_ref[i, 0:64] = keys[i * 64 : (i + 1) * 64]
        kv_ref[i, 64:128] = values[i * 64 : (i + 1) * 64]

    @pl.when(g == c)
    def _():
        all_ref[own_line, tp, 0:128] = kv_ref[g]

    pl.semaphore_wait(barrier, len(peers))

    def decay_copy(k):
        t = lax.rem(mine + k, 4)
        peer = (z, y, 2 * g + t // 2, lax.rem(t, 2))
        return remote(d_ref, dec_ref.at[mine], d_send.at[k], d_recv.at[k], peer)

    def piece_copy(k):
        to = lax.rem(x + k, 4)
        slot = (x - 2 * g) * 2 + c
        return remote(
            kv_ref.at[to // 2],
            all_ref.at[own_line, tp, pl.ds(0, 128)],
            p_send.at[k],
            p_recv.at[slot],
            (z, y, to, g),
        )

    for k in range(1, 4):
        decay_copy(k).start()
    for k in range(1, 4):
        piece_copy(k).start()

    @pl.when(g != c)
    def _():
        piece_copy(0).start()

    def queries(slot):
        flat = jnp.dot(norm_ref[...], wq_ref[slot], preferred_element_type=f32)
        return (head_norm(flat.T, 8, gain) * (LOG2E / 8)).astype(bf)

    far_copy.wait()
    qs_ref[...] = queries(0)

    for k in range(1, 4):
        decay_copy(k).wait_recv()
    for i in range(4):
        first = pl.multiple_of((4 * c + i) * 128, 128)
        value = jnp.concatenate([dec_ref[q, :, pl.ds(first, 128)] for q in range(4)], axis=0)
        all_ref[own_line, 4 * c + i, 128:152] = jnp.concatenate(
            split3(value * LOG2E), axis=0
        ).astype(bf)
    far_first = pl.multiple_of((7 - tp) * 128, 128)
    far_decays = remote(
        dec_ref.at[:, :, pl.ds(far_first, 128)], far_ref, x_send.at[0], x_recv.at[0], across
    )
    far_decays.start()
    q_copy = remote(qs_ref, qr_ref, x_send.at[1], x_recv.at[1], mirror)
    late = own_line < 8

    @pl.when(jnp.logical_not(late))
    def _():
        q_copy.start()

    def block(line, sub):
        return all_ref.at[line, pl.ds(4 * c + 2 * sub, 2)]

    def ring(step, slot):
        side = (0, 0, 0, 0, 3, 1)[slot]
        sub = (0, 1, 0, 1, 0, 1)[slot]
        upward = slot in (0, 1, 4)
        if step == 0:
            line, peer = line_at(side, 0), (up_a if upward else down_a)
        else:
            line, peer = line_at(step - 1, side), (up_b if upward else down_b)
        index = step * 6 + slot
        ref = block(line, sub)
        return remote(ref, ref, r_send.at[index], r_recv.at[index], peer)

    def share(j, k):
        half = all_ref.at[line_at(j, k), pl.ds(4 * c, 4)]
        index = j * 4 + k
        return remote(half, half, s_send.at[index], s_recv.at[index], sibling)

    def ring_start(step):
        for slot in range(4):
            ring(step, slot).start()

    def ring_relay(step):
        ring(step, 0).wait_recv()
        ring(step, 4).start()
        ring(step, 3).wait_recv()
        ring(step, 5).start()
        ring(step, 1).wait_recv()
        ring(step, 2).wait_recv()

    def ring_end(step):
        ring(step, 4).wait_recv()
        ring(step, 5).wait_recv()

    for i in range(4):

        @pl.when(4 * c + i != tp)
        def _():
            remote(
                kv_ref.at[0],
                all_ref.at[own_line, 4 * c + i, pl.ds(0, 128)],
                p_send.at[0],
                p_recv.at[i],
                sibling,
            ).wait_recv()

    ring_start(0)
    ring_start(1)
    share(0, 0).start()

    row8 = lax.broadcasted_iota(jnp.int32, (8, 128), 0)
    ones = jnp.where(row8 < 3, 1.0, 0.0).astype(f32)

    def prepare(rg, query_ref, decays):
        ref_d = jnp.broadcast_to(decays[:, 0:1], (8, 128))
        refd_ref[rg] = ref_d
        parts = split3(decays - ref_d)
        for h in range(8):
            onehot = jnp.where(row8 == h, -1.0, 0.0).astype(f32)
            own = jnp.zeros((8, 128), f32)
            for i, part in enumerate(parts):
                own = jnp.where(row8 == i, part[h : h + 1], own)
            rows = jnp.concatenate([onehot, onehot, onehot, own], axis=0).astype(bf)
            qa_ref[rg, :, h * 128 : (h + 1) * 128] = jnp.concatenate(
                [query_ref[h * 64 : (h + 1) * 64, :], rows, jnp.zeros((32, 128), bf)], axis=0
            )

    near_copy.wait()
    out_copy.start()
    near_ref[...] = queries(1)
    here = pl.multiple_of(tp * 128, 128)
    own_decays = jnp.concatenate([dec_ref[q, :, pl.ds(here, 128)] for q in range(4)], axis=0)
    prepare(0, near_ref, own_decays * LOG2E)
    acc_ref[...] = jnp.zeros_like(acc_ref)
    sum_ref[...] = jnp.zeros_like(sum_ref)
    if not bounded:
        max_ref[...] = jnp.full(max_ref.shape, -1e30, f32)

    def attend(parts, tp_row, masked):
        for i, (rg, line) in enumerate(parts):
            ref_d = refd_ref[rg]
            for p in range(8):
                first = i * 1024 + p * 128
                ka_ref[first : first + 128] = load_keys(all_ref, line, p, ref_d, ones)
        units = [
            (i, m, n)
            for i in range(len(parts))
            for m in range(1024 // ROWS)
            for n in range(1024 // tile)
        ]

        def weigh(u):
            i, m, n = units[u]
            rg = parts[i][0]
            cols = slice(n * tile, (n + 1) * tile)
            first = i * 1024 + m * ROWS
            keys = ka_ref[first : first + ROWS]
            scores = jnp.dot(keys, qa_ref[rg, :, cols], preferred_element_type=f32)
            if masked:
                shape = (ROWS, tile)
                key_pos = m * ROWS + lax.broadcasted_iota(jnp.int32, shape, 0)
                query_pos = tp_row * 128 + (lax.broadcasted_iota(jnp.int32, shape, 1) & 127)
                scores = jnp.where(key_pos <= query_pos, scores, -1e30)
            if bounded:
                weights = jnp.exp2(scores)
                sum_ref[rg, :, cols] += jnp.sum(weights.reshape(ROWS // 8, 8, tile), axis=0)
            else:
                old = max_ref[rg, 0:1, cols]
                new = jnp.maximum(old, jnp.max(scores, axis=0, keepdims=True))
                keep = jnp.exp2(old - new)
                weights = jnp.exp2(scores - new)
                max_ref[rg, :, cols] = jnp.broadcast_to(new, (8, tile))
                sums = jnp.sum(weights.reshape(ROWS // 8, 8, tile), axis=0)
                sum_ref[rg, :, cols] = sum_ref[rg, :, cols] * keep + sums
                acc_ref[rg, :, cols] = acc_ref[rg, :, cols] * keep
            wt_ref[u % (lag + 1)] = weights.astype(bf)

        def gather_values(u):
            i, m, n = units[u]
            rg, line = parts[i]
            cols = slice(n * tile, (n + 1) * tile)
            first = m * ROWS // 128
            values = jnp.concatenate(
                [all_ref[line, p, 64:128] for p in range(first, first + ROWS // 128)], axis=1
            )
            acc_ref[rg, :, cols] += jnp.dot(
                values, wt_ref[u % (lag + 1)], preferred_element_type=f32
            )

        lag = LAG if bounded else 0
        for u in range(len(units) + lag):
            if u < len(units):
                weigh(u)
            if u >= lag:
                gather_values(u - lag)

    def got(step, slot):
        ring(step, slot).wait_recv()

    def pass_on(step, sub):
        for slot in (sub, 2 + sub):
            ring(step, slot).start()

    def act_1():
        got(0, 0)
        ring(0, 4).start()
        pass_on(4, 0)
        got(0, 2)
        pass_on(2, 0)
        got(1, 0)
        ring(1, 4).start()
        got(0, 3)
        ring(0, 5).start()
        pass_on(2, 1)
        got(0, 1)
        pass_on(4, 1)
        share(3, 0).start()
        share(1, 0).start()
        got(1, 3)
        ring(1, 5).start()
        got(1, 1)
        got(1, 2)
        share(0, 3).start()
        share(0, 1).start()

    def act_3():
        got(0, 4)
        pass_on(3, 0)
        got(0, 5)
        pass_on(3, 1)
        share(2, 0).start()
        ring_end(1)
        share(0, 2).start()

    def act_6():
        got(4, 0)
        ring(4, 4).start()
        got(2, 0)
        ring(2, 4).start()
        got(2, 3)
        ring(2, 5).start()
        got(2, 1)
        got(2, 2)
        share(1, 3).start()
        share(1, 1).start()
        got(4, 3)
        ring(4, 5).start()
        got(4, 1)
        got(4, 2)
        share(3, 3).start()
        share(3, 1).start()

        @pl.when(late)
        def _():
            q_copy.start()

    def act_9():
        ring_relay(3)
        share(2, 3).start()
        share(2, 1).start()
        for j in (3, 1):
            ring_end(1 + j)
            share(j, 2).start()

    def act_13():
        ring_end(3)
        share(2, 2).start()

    later = jnp.where(late, 0, 1)
    one = lambda test: test.astype(jnp.int32)

    def wait_half(j, k):
        half = all_ref.at[line_at(j, k), pl.ds(4 * (1 - c), 4)]
        index = k * 4 + j
        remote(half, half, s_send.at[index], s_recv.at[index], sibling).wait_recv()

    far_line = 15 - own_line
    last_line = line_at(2, 2)
    early = jnp.logical_not(late) & (last_line > far_line)
    hold = jnp.logical_not(late) & (last_line <= far_line)

    def back(part):
        rows = pl.ds(part * 256, 256)
        return remote(
            os_ref.at[rows], got_ref.at[rows], x_send.at[2 + part], x_recv.at[2 + part], mirror
        )

    def finish(rg, to_ref):
        inverse = 1.0 / jnp.sum(sum_ref[rg], axis=0, keepdims=True)
        for h in range(8):
            cols = slice(h * 128, (h + 1) * 128)
            to_ref[h * 64 : (h + 1) * 64, :] = (acc_ref[rg, :, cols] * inverse[:, cols]).astype(bf)

    wait_half(0, 0)
    attend([(0, own_line)], tp, True)

    def body(group, carry):
        actions = ((0, act_1), (1 + later, act_3), (2 + later, act_6), (5, act_9), (6 + one(early), act_13))
        for at, action in actions:

            @pl.when(group == at)
            def _(action=action):
                action()

        @pl.when(group == jnp.where(late, 99, 6 + one(hold)))
        def _():
            for part in range(2):
                back(part).start()

        for at, members in enumerate(GROUPS):

            @pl.when(group == (at + one(early) if at == 6 else at))
            def _(members=members):
                for j, k in members:
                    if (j, k) != (0, 0):
                        wait_half(j, k)

        @pl.when(group == 5 * later)
        def _():
            far_decays.wait_recv()
            q_copy.wait_recv()
            far = jnp.concatenate([far_ref[q] for q in range(4)], axis=0)
            prepare(1, qr_ref, far * LOG2E)

        turn = group + later * (2 * one(group == 5) - one(group > 5) * one(early))
        turn = turn - 2 * one(hold) * one(group == 7)
        again = one(turn == 7)
        size = unpacked((3, 2, 2, 2, 2, 4, 1, 0), turn)
        lines = []
        for i in range(4):
            pick = lambda axis: unpacked(
                [g[i][axis] if i < len(g) else 0 for g in GROUPS] + [0], turn
            )
            lines.append(line_at(pick(0), pick(1)))
        flags = []
        for i in range(4):
            here = one(i < size)
            flags.append(here * one(lines[i] < own_line) * (1 - one(hold) * one(group == 6)))
            flags.append(here * one(lines[i] < far_line) * jnp.where(turn == 6, 1, 1 - later))
        lines.append(last_line)
        flags.append(one(last_line < own_line) * one(hold) * one(group == 7))
        before, count = [], 0
        for flag in flags:
            before.append(count)
            count = count + flag
        count = count * (1 - again) + (far_line - one(last_line < far_line)) * again

        def unit(index):
            rg, line = again, (index + one(index >= last_line)) * again
            for i in range(9):
                chosen = flags[i] * one(before[i] == index)
                line = line + chosen * lines[i // 2]
                if i % 2:
                    rg = rg + chosen
            return rg, line

        def pair(index, inner):
            attend([unit(2 * index), unit(2 * index + 1)], tp, False)
            return inner

        lax.fori_loop(0, count // 2, pair, 0)

        @pl.when((count & 1) == 1)
        def _():
            attend([unit(count - 1)], tp, False)

        @pl.when(group == 4 + later)
        def _():
            attend([(1, far_line)], 7 - tp, True)

        @pl.when(group == jnp.where(late, 99, 5 + one(hold)))
        def _():
            finish(1, os_ref)

        return carry

    lax.fori_loop(0, 7 + later, body, 0)

    @pl.when(late)
    def _():
        finish(1, os_ref)

    finish(0, near_ref)

    @pl.when(late)
    def _():
        for part in range(2):
            back(part).start()

    out_copy.wait()
    near = near_ref[...].T
    for n in range(4):
        cols = slice(n * 512, (n + 1) * 512)
        part_ref[:, cols] = jnp.dot(near, wo_ref[pl.ds(w_near, 512), cols], preferred_element_type=f32)
    for k in range(1, 4):
        decay_copy(k).wait_send()
        piece_copy(k).wait_send()

    @pl.when(g != c)
    def _():
        piece_copy(0).wait_send()

    far_decays.wait_send()
    q_copy.wait_send()
    for step in range(5):
        for slot in range(6):
            ring(step, slot).wait_send()
    for j in range(4):
        for k in range(4):
            share(j, k).wait_send()
    for part in range(2):
        back(part).wait_recv()
        far = got_ref[part * 256 : (part + 1) * 256, :].T
        rows = pl.ds(pl.multiple_of(w_far + part * 256, 256), 256)
        for n in range(2):
            cols = slice(n * 1024, (n + 1) * 1024)
            rest = jnp.dot(far, wo_ref[rows, cols], preferred_element_type=f32)
            if part == 0:
                part_ref[:, cols] += rest
            else:
                out_ref[:, cols] = (part_ref[:, cols] + rest).astype(bf)
    for part in range(2):
        back(part).wait_send()


def main(x, in_gain, wk, wv, qg, kg, d, wq, wo, bounded):
    dma = lambda *n: pltpu.SemaphoreType.DMA(n)
    return pl.pallas_call(
        functools.partial(main_kernel, bounded, 512),
        out_shape=[jax.ShapeDtypeStruct((128, 2048), bf), jax.ShapeDtypeStruct((1,), f32)],
        in_specs=[HBM, VM, HBM, HBM, VM, VM, VM, HBM, HBM],
        out_specs=[VM, pl.BlockSpec(memory_space=pltpu.SMEM)],
        scratch_shapes=[
            pltpu.VMEM((128, 2048), bf),
            pltpu.VMEM((2048, 128), bf),
            pltpu.VMEM((2048, 128), bf),
            pltpu.VMEM((128, 2048), bf),
            pltpu.VMEM((2, 128, 128), bf),
            pltpu.VMEM((16, 8, 152, 128), bf),
            pltpu.VMEM((4, 2, 1024), f32),
            pltpu.VMEM((4, 2, 128), f32),
            pltpu.VMEM((2, 2048, 512), bf),
            pltpu.VMEM((1024, 2048), bf),
            pltpu.VMEM((128, 2048), f32),
            pltpu.VMEM((512, 128), bf),
            pltpu.VMEM((512, 128), bf),
            pltpu.VMEM((512, 128), bf),
            pltpu.VMEM((512, 128), bf),
            pltpu.VMEM((512, 128), bf),
            pltpu.VMEM((2, 128, 1024), bf),
            pltpu.VMEM((2, 64, 1024), f32),
            pltpu.VMEM((2, 8, 1024), f32),
            pltpu.VMEM((2, 8, 1024), f32),
            pltpu.VMEM((2, 8, 128), f32),
            pltpu.VMEM((2048, 128), bf),
            pltpu.VMEM((LAG + 1, ROWS, 512), bf),
            dma(6),
            dma(4),
            dma(4),
            dma(4),
            dma(4),
            dma(4),
            dma(4),
            dma(30),
            dma(30),
            dma(16),
            dma(16),
        ],
        compiler_params=pltpu.CompilerParams(
            collective_id=0 if bounded else 1,
            has_side_effects=True,
            vmem_limit_bytes=60 * 1024 * 1024,
        ),
        name="main_bounded" if bounded else "main_any",
    )(x, in_gain, wk, wv, qg, kg, d, wq, wo)


def per_device(inputs, in_gain, w_query, w_key, w_value, query_gain, key_gain, decay_sums, w_out):
    args = (
        inputs,
        in_gain.reshape(1, -1),
        w_key,
        w_value,
        query_gain.reshape(1, -1),
        key_gain.reshape(1, -1),
        decay_sums.T,
        w_query,
        w_out,
    )
    result, bound = main(*args, True)
    return lax.cond(
        bound[0] <= 64.0, lambda kept, *a: kept, lambda kept, *a: main(*a, False)[0], result, *args
    )


def solution(mesh):
    torus = Mesh(mesh.devices.reshape(4, 4, 4, 2), ("z", "y", "x", "c"))
    every = ("z", "y", "x", "c")
    in_specs = (P(every, None), P(), P(), P(), P(), P(), P(), P(("z", "y"), ("x", "c")), P())
    return jax.shard_map(
        per_device, mesh=torus, in_specs=in_specs, out_specs=P(every, None), check_vma=False
    )
```
